256 devices in a mesh: grp: 2 (over z), ep: 16 (over y, core), tp: 8 (over x).
Axes of the slice: x: 8, y: 8, z: 2, core: 2. Of those that a mesh axis runs over, the one named last changes fastest.
The devices are a block of a 8x8x16 slice.
Arguments:
- tokens: bfloat16 [4096, 4096], P(('grp', 'ep'), 'tp'), parts along dimension 0, may hold values from -6 to 6
- routes: int32 [4096, 4], P(('grp', 'ep')), parts along dimension 0, may hold values from 0 to 15, all different within a row; in each aligned block of 128 rows (0 to 127, 128 to 255, ...) at most 64 rows name the same one
- route_weights: float32 [4096, 4], P(('grp', 'ep')), parts along dimension 0, may hold values from 0.1 to 1
- norm_gain: float32 [4096], replicated, may hold values from 0.1 to 1.9
- expert_gate: bfloat16 [16, 4096, 1024], P('ep', 'tp'), may hold values from -0.09375 to 0.09375
- expert_up: bfloat16 [16, 4096, 1024], P('ep', 'tp'), may hold values from -0.09375 to 0.09375
- expert_down: bfloat16 [16, 1024, 4096], P('ep', None, 'tp')
- shared_gate: bfloat16 [4096, 1024], P('tp'), may hold values from -0.09375 to 0.09375
- shared_up: bfloat16 [4096, 1024], P('tp'), may hold values from -0.09375 to 0.09375
- shared_down: bfloat16 [1024, 4096], P(None, 'tp')
- out_gain: float32 [4096], P('tp'), may hold values from 0.1 to 1.9
Outputs:
- layer_out: bfloat16 [4096, 4096], P(('grp', 'ep'), 'tp'), parts along dimension 0
The draws below stay inside these ranges and needn't reach their ends.
There are 2 independent parts, one for each index of `grp`. The reference program is written for one: setup_inputs(seed, part) draws one part's arguments, and reference() takes and returns one part's arrays. A program takes and returns all parts, laid end to end along the dimension named above; an argument that names none is the same for every part. Nothing has to cross between parts.
Inputs may be any that keep to these rules, and one draw needn't show every extreme that they name: `routes`: each row names 4 different experts; among the rows of one index of ep no expert is named more than 64 times, and in some such block some expert is named exactly 64 times.
All inputs are finite; a program needn't handle non-finite values.
Results may differ from the reference program's by a relative error of at most 0.023.
Values may be sent and summed in bfloat16 or wider, within the bound.
No kernel may reach another device: no remote copies, remote signals or barrier semaphores. Data moves between devices by JAX's collectives and lax.ppermute only.
A program may use at most 64 MiB of HBM per device.

```python
import math
import jax
import jax.numpy as jnp
import numpy as np
from jax import lax

D = 4096
FF = 1024
FS = 1024
TOP_K = 4
TOK_EP = 128
EXPERTS = 16
CAP = 64
TOKENS = 2048
N_TP = 8


def rising_columns(key, width):
    base = jnp.exp(jnp.linspace(0.0, math.log(4.0), width, dtype=jnp.float32))
    jitter = jax.random.uniform(key, (width,), jnp.float32, 0.8, 1.2)
    return base * jitter


def draw_expert_down(key, part):
    noise = jax.random.normal(jax.random.fold_in(key, 11), (EXPERTS, FF, D), jnp.float32)
    rise = rising_columns(jax.random.fold_in(key, 12), D)
    return (noise * rise * FF ** (-0.5)).astype(jnp.bfloat16)


def draw_shared_down(key, part):
    noise = jax.random.normal(jax.random.fold_in(key, 21), (FS, D), jnp.float32)
    rise = rising_columns(jax.random.fold_in(key, 22), D)
    return (noise * rise * FS ** (-0.5)).astype(jnp.bfloat16)


def level_of(rng, extent, pieces, least, high):
    level = 1.0
    for position, shards_of in pieces:
        steps = jax.random.uniform(jax.random.fold_in(jax.random.fold_in(rng, 6), position), (shards_of,), jnp.float32, least / len(pieces), high / len(pieces))
        level = level * jnp.repeat(jnp.exp(steps), extent[position] // shards_of).reshape((-1,) + (1,) * (len(extent) - 1 - position))
    return level


def shared_out(own_key, own, number, rows, count, top, reach, lean):
    sequence = jax.random.permutation(own_key, count)
    crowded, usual = load_shares(count, rows * top, reach, lean, True), load_shares(count, rows * top, reach, lean, False)
    places = jnp.arange(count)

    def named(sizes, rotation):
        used = int((sizes > 0).sum())
        fixed = max(1, used // 4)
        shifted = fixed + (places - fixed + rotation * (used - fixed)) % max(1, count - fixed)
        return jnp.zeros((count,), jnp.int32).at[sequence[jnp.where(places < fixed, places, shifted)]].set(jnp.asarray(sizes, jnp.int32))

    sizes = jnp.where(number % 4 == 0, named(crowded, number // 4), named(usual, number - number // 4 - 1))
    mixed = jax.random.permutation(jax.random.fold_in(own, 3), count)
    giver, receiver = mixed[0:count // 2 * 2:2], mixed[1:count // 2 * 2:2]
    room = jnp.minimum(sizes[giver] - 1, reach - sizes[receiver]) // 2
    room = jnp.where((giver == sequence[0]) | (receiver == sequence[0]) | (sizes[receiver] == 0), 0, jnp.maximum(room, 0))
    shifted = jax.random.randint(jax.random.fold_in(own, 4), (count // 2,), 0, 1 << 20) % (room + 1)
    sizes = sizes.at[giver].add(-shifted).at[receiver].add(shifted)
    labels = jnp.searchsorted(jnp.cumsum(sizes), jnp.arange(rows * top), side="right").astype(jnp.int32)
    table = labels.reshape(top, rows).T
    table = table[jax.random.permutation(jax.random.fold_in(own, 1), rows)]
    rotation = jax.random.randint(jax.random.fold_in(own, 2), (rows, 1), 0, top)
    return jnp.take_along_axis(table, (jnp.arange(top)[None, :] + rotation) % top, axis=1)


def load_shares(number_of, total, reach, slope, full):
    portions = [(1 << 20) // math.isqrt(rank ** slope) + 1 for rank in range(1, number_of + 1)]
    largest = reach if full else min(reach, max(-(-total // number_of), total * portions[0] // sum(portions)))
    least = 1 if total - largest >= number_of - 1 else 0
    counts, surplus = [largest] + [least] * (number_of - 1), total - largest - least * (number_of - 1)
    while surplus > 0:
        candidates = [i for i in range(1, number_of) if counts[i] < largest] or [i for i in range(1, number_of) if counts[i] < reach]
        pool, remaining = sum([portions[i] for i in candidates]), surplus
        for i in candidates:
            more = min(reach - counts[i], max(1, remaining * portions[i] // pool), surplus)
            counts[i] = counts[i] + more
            surplus = surplus - more
    return np.array(counts)


def normal_values(rng, shape, deviation, reach, split=(), kind=jnp.bfloat16):
    gain = level_of(rng, shape, split, -0.22, 0.18) if split else 1.0
    values = jax.random.normal(rng, shape, jnp.float32) * deviation * gain
    return jnp.minimum(jnp.maximum(values, -reach), reach).astype(kind)


def setup_inputs(seed: int = 0, part: int = 0) -> dict:
    key_of = jax.random.split(jax.random.key(seed), 12)
    part_keys = jax.random.split(jax.random.fold_in(key_of[11], part), 12)
    tokens = normal_values(part_keys[0], (TOKENS, D), 1.0, 6.0, ((0, 16), (1, 8)))
    routes_keys = jax.random.split(jax.random.fold_in(part_keys[1], 1), TOKENS // TOK_EP)
    routes_turns = jax.random.permutation(jax.random.fold_in(part_keys[1], 3), TOKENS // TOK_EP)
    routes = jax.vmap(lambda own, number: shared_out(jax.random.fold_in(part_keys[1], 2), own, number, TOK_EP, EXPERTS, TOP_K, CAP, 2))(routes_keys, routes_turns).reshape((TOKENS, TOP_K))
    route_weights = jnp.clip(jnp.exp(math.log(1.0) - 2.3025851 * jax.random.uniform(part_keys[2], (TOKENS, TOP_K), jnp.float32) ** level_of(part_keys[2], (TOKENS, TOP_K), ((0, 16),), -0.2, 0.2)), 0.1, 1.0)
    norm_gain = jnp.clip(1.0 + 0.18 * jax.random.normal(key_of[3], (D,), jnp.float32), 0.1, 1.9)
    expert_gate = normal_values(key_of[4], (EXPERTS, D, FF), D ** -0.5, 0.09375, ((0, 16), (1, 8)))
    expert_up = normal_values(key_of[5], (EXPERTS, D, FF), D ** -0.5, 0.09375, ((0, 16), (1, 8)))
    expert_down = draw_expert_down(jax.random.fold_in(key_of[11], 71), part)
    shared_gate = normal_values(key_of[7], (D, FS), D ** -0.5, 0.09375, ((0, 8),))
    shared_up = normal_values(key_of[8], (D, FS), D ** -0.5, 0.09375, ((0, 8),))
    shared_down = draw_shared_down(jax.random.fold_in(key_of[11], 71), part)
    out_gain = jnp.clip(1.0 + 0.18 * jax.random.normal(key_of[10], (D,), jnp.float32), 0.1, 1.9)
    return dict(tokens=tokens, routes=routes, route_weights=route_weights, norm_gain=norm_gain, expert_gate=expert_gate, expert_up=expert_up, expert_down=expert_down, shared_gate=shared_gate, shared_up=shared_up, shared_down=shared_down, out_gain=out_gain)


epsilon = 1e-06

def blocked_product(source, matrix):
    rows = source.shape[0]
    source_blocks = source.reshape(rows, N_TP, -1).astype(jnp.float32)
    matrix_blocks = matrix.reshape(N_TP, -1, matrix.shape[1]).astype(jnp.float32)
    partial_value = jnp.einsum('rbf,bfh->brh', source_blocks, matrix_blocks)
    rounded = lax.optimization_barrier(partial_value.astype(jnp.bfloat16))
    return lax.optimization_barrier(jnp.sum(rounded.astype(jnp.float32), axis=0))

def expert_hidden(source, gate_matrix, up_matrix):
    gate_part = blocked_product(source, gate_matrix)
    up_part = blocked_product(source, up_matrix)
    return (jax.nn.silu(gate_part) * up_part).astype(jnp.bfloat16)

def reference(tokens, routes, route_weights, norm_gain, expert_gate, expert_up, expert_down, shared_gate, shared_up, shared_down, out_gain):
    full_float = tokens.astype(jnp.float32)
    normed = (full_float * lax.rsqrt(lax.optimization_barrier(jnp.mean(full_float * full_float, axis=-1, keepdims=True)) + epsilon) * norm_gain).astype(jnp.bfloat16)
    choose = (routes[:, :, None] == jnp.arange(EXPERTS, dtype=jnp.int32)[None, None, :]).astype(jnp.float32)
    weight_table = lax.optimization_barrier(jnp.sum(route_weights[:, :, None] * choose, axis=1))

    def add_expert(totals, expert):
        hidden = expert_hidden(normed, expert_gate[expert], expert_up[expert])
        expert_rows = jnp.dot(hidden, expert_down[expert], preferred_element_type=jnp.float32).astype(jnp.bfloat16)
        column = lax.dynamic_slice_in_dim(weight_table, expert, 1, 1)
        return (totals + column * expert_rows.astype(jnp.float32), None)
    routed, _ = lax.scan(add_expert, jnp.zeros((normed.shape[0], D), jnp.float32), jnp.arange(EXPERTS, dtype=jnp.int32))
    shared_hidden = expert_hidden(normed, shared_gate, shared_up)
    mixture = routed + jnp.dot(shared_hidden, shared_down, preferred_element_type=jnp.float32)
    scale = lax.rsqrt(lax.optimization_barrier(jnp.mean(mixture * mixture, axis=-1, keepdims=True)) + epsilon)
    return (mixture * scale * out_gain).astype(jnp.bfloat16)
```

```python
import jax
import jax.numpy as jnp
from jax import lax
from jax.sharding import PartitionSpec as P

epsilon = 1e-06
f32 = jnp.float32
bf16 = jnp.bfloat16


def dot(a, b):
    return jnp.dot(a, b, preferred_element_type=f32)


def ring(count, step):
    return [(i, (i + step) % count) for i in range(count)]


def turned(blocks, first):
    count = blocks.shape[0]
    return lax.dynamic_slice_in_dim(jnp.concatenate([blocks, blocks], 0), first, count, 0)


def reduce_scatter(piece, size, long_way, axis):
    half = size // 2
    ahead, back = ring(size, 1), ring(size, -1)
    f_len, b_len = (half, size - 1 - half) if long_way > 0 else (size - 1 - half, half)
    f = b = None
    for d in range(half, 0, -1):
        if d <= f_len:
            own = piece(d)
            f = lax.ppermute(own if f is None else (own.astype(f32) + f.astype(f32)).astype(bf16), axis, ahead)
        if d <= b_len:
            own = piece(-d)
            b = lax.ppermute(own if b is None else (own.astype(f32) + b.astype(f32)).astype(bf16), axis, back)
    return piece(0).astype(f32) + f.astype(f32) + b.astype(f32)


def all_gather(block, size, long_way, axis):
    half = size // 2
    ahead, back = ring(size, 1), ring(size, -1)
    f_len, b_len = (half, size - 1 - half) if long_way > 0 else (size - 1 - half, half)
    out = {0: block}
    f = b = block
    for d in range(1, half + 1):
        if d <= f_len:
            f = lax.ppermute(f, axis, ahead)
            out[size - d] = f
        if d <= b_len:
            b = lax.ppermute(b, axis, back)
            out[d] = b
    return [out[d] for d in range(size)]


def per_device(
    tokens,
    routes,
    route_weights,
    norm_gain,
    expert_gate,
    expert_up,
    expert_down,
    shared_gate,
    shared_up,
    shared_down,
    out_gain,
):
    tok_count, width = tokens.shape
    tp = lax.axis_size("tp")
    experts = lax.axis_size("ep")
    chips = experts // 2
    full_width = width * tp
    me_tp = lax.axis_index("tp")
    me_ep = lax.axis_index("ep")
    top_count = routes.shape[1]
    capacity = min(tok_count, 2 * tok_count * top_count // experts)
    gain = lax.dynamic_slice_in_dim(norm_gain, me_tp * width, width, 0)
    gate_matrix, up_matrix, down_matrix = expert_gate[0], expert_up[0], expert_down[0]
    hidden_units = gate_matrix.shape[1]

    ahead = ring(experts, 2)
    back = ring(experts, -2)
    partner = [(i, i ^ 1) for i in range(experts)]

    weight_high = route_weights.astype(bf16)
    weight_low = (route_weights - weight_high.astype(f32)).astype(bf16)
    info = jnp.concatenate([routes.astype(bf16), weight_high, weight_low], 1)
    info = jnp.pad(info, ((0, 0), (0, 128 - info.shape[1])))
    packet = jnp.concatenate([tokens, info], 1)
    got = {0: packet}
    f = b = packet
    half = chips // 2
    for d in range(1, half + 1):
        f = lax.ppermute(f, "ep", ahead)
        got[-d] = f
        if d < chips - d:
            b = lax.ppermute(b, "ep", back)
            got[d] = b
    near = [0, -1, 1]
    far = [k for d in range(2, half) for k in (-d, d)] + [-half]

    def arrived(places):
        mine = jnp.stack([got[k] for k in places])
        theirs = lax.ppermute(mine, "ep", partner)
        return jnp.concatenate([mine, theirs], 0)

    upper = (
        lax.broadcasted_iota(jnp.int32, (tok_count, tok_count), 0)
        <= lax.broadcasted_iota(jnp.int32, (tok_count, tok_count), 1)
    ).astype(bf16)

    def picked(packets):
        table = packets[:, :, width:].astype(f32)
        hit = table[:, :, :top_count] == me_ep.astype(f32)
        weight = table[:, :, top_count : 2 * top_count] + table[:, :, 2 * top_count : 3 * top_count]
        weight = jnp.sum(jnp.where(hit, weight, 0.0), axis=2)
        routed = jnp.any(hit, axis=2)
        place = dot(routed.astype(bf16), upper) - 1.0
        place = jnp.where(routed, place, -1.0)
        slots = lax.broadcasted_iota(jnp.int32, (1, capacity, 1), 1).astype(f32)
        pick = (place[:, None, :] == slots).astype(bf16)
        rows = jnp.einsum("bst,btk->bsk", pick, packets[:, :, :width], preferred_element_type=f32)
        return rows, pick, weight

    def partials(rows, gate, up):
        rows = rows.astype(f32)
        squares = jnp.sum(rows * rows, axis=1, keepdims=True)
        squares = jnp.broadcast_to(squares, (rows.shape[0], 128)).astype(bf16)
        scaled = (rows * gain).astype(bf16)
        both = jnp.concatenate([scaled, squares], 1)
        both = turned(both.reshape(tp, -1, both.shape[1]), me_tp).reshape(rows.shape[0], -1)
        scaled, squares = both[:, :width], both[:, width:]
        gate_part = dot(scaled, gate).astype(bf16)
        up_part = dot(scaled, up).astype(bf16)
        return [v.reshape(tp, -1, v.shape[1]) for v in (gate_part, up_part, squares)]

    def hidden_of(total):
        scale = lax.rsqrt(total[:, 2 * hidden_units : 2 * hidden_units + 1] / full_width + epsilon)
        gate_value = total[:, :hidden_units] * scale
        up_value = total[:, hidden_units : 2 * hidden_units] * scale
        return (jax.nn.silu(gate_value) * up_value).astype(bf16)

    def unturned(rows):
        return turned(rows.reshape(tp, -1, rows.shape[1]), (tp - me_tp) % tp).reshape(rows.shape)

    def to_tokens(hidden, pick, weight):
        expert_rows = unturned(dot(hidden, down_matrix).astype(bf16))
        expert_rows = expert_rows.reshape(-1, capacity, width)
        spread = jnp.einsum("bst,bsk->btk", pick, expert_rows, preferred_element_type=f32)
        return spread * weight[:, :, None]

    near_rows, near_pick, near_weight = picked(arrived(near))
    far_rows, far_pick, far_weight = picked(arrived(far))

    shared_parts = partials(tokens, shared_gate, shared_up)
    near_parts = partials(near_rows.reshape(-1, width), gate_matrix, up_matrix)
    far_parts = partials(far_rows.reshape(-1, width), gate_matrix, up_matrix)

    def near_piece(d):
        return jnp.concatenate(
            [jnp.concatenate([v[d % tp] for v in parts], 1) for parts in (shared_parts, near_parts)], 0
        )

    def far_piece(d):
        return jnp.concatenate([v[d % tp] for v in far_parts], 1)

    near_hidden = hidden_of(reduce_scatter(near_piece, tp, 1, "tp"))
    far_hidden = hidden_of(reduce_scatter(far_piece, tp, -1, "tp"))
    far_all = jnp.concatenate(all_gather(far_hidden, tp, 1, "tp"), 0)
    near_all = all_gather(near_hidden, tp, -1, "tp")
    shared_rows = tok_count // tp
    shared_all = jnp.concatenate([v[:shared_rows] for v in near_all], 0)
    near_all = jnp.concatenate([v[shared_rows:] for v in near_all], 0)

    def chip_sums(places, values):
        count = len(places)
        theirs = lax.ppermute(values[count:].astype(bf16), "ep", partner)
        total = values[:count] + theirs.astype(f32)
        return {k: total[i] for i, k in enumerate(places)}

    far_sums = chip_sums(far, to_tokens(far_all, far_pick, far_weight))
    shared_out = unturned(dot(shared_all, shared_down))
    near_sums = chip_sums(near, to_tokens(near_all, near_pick, near_weight))

    sums = {**far_sums, **near_sums}
    cut = width // 2
    f = lax.ppermute(sums[-half][:, :cut].astype(bf16), "ep", ahead).astype(f32)
    b = lax.ppermute(sums[-half][:, cut:].astype(bf16), "ep", back).astype(f32)
    f = jnp.concatenate([f, jnp.zeros_like(f)], 1)
    b = jnp.concatenate([jnp.zeros_like(b), b], 1)
    for d in range(half - 1, 0, -1):
        f = lax.ppermute((sums[d] + f).astype(bf16), "ep", ahead).astype(f32)
        b = lax.ppermute((sums[-d] + b).astype(bf16), "ep", back).astype(f32)
    mixture = sums[0] + f + b + shared_out

    square_sum = jnp.sum(mixture * mixture, axis=-1)
    step = 1
    while step < tp:
        square_sum = square_sum + lax.ppermute(square_sum, "tp", [(i, i ^ step) for i in range(tp)])
        step *= 2
    scale = lax.rsqrt(square_sum / full_width + epsilon)
    return (mixture * scale[:, None] * out_gain).astype(bf16)


def solution(mesh):
    return jax.shard_map(
        per_device,
        mesh=mesh,
        in_specs=(
            P(("grp", "ep"), "tp"),
            P(("grp", "ep"), None),
            P(("grp", "ep"), None),
            P(),
            P("ep", "tp", None),
            P("ep", "tp", None),
            P("ep", None, "tp"),
            P("tp", None),
            P("tp", None),
            P(None, "tp"),
            P("tp"),
        ),
        out_specs=P(("grp", "ep"), "tp"),
        check_vma=False,
    )
```

```python
import jax
import jax.numpy as jnp
from jax import lax
from jax.sharding import PartitionSpec as P

epsilon = 1e-06
f32 = jnp.float32
bf16 = jnp.bfloat16


def dot(a, b):
    return jnp.dot(a, b, preferred_element_type=f32)


def ring(count, step):
    return [(i, (i + step) % count) for i in range(count)]


def turned(blocks, first):
    count = blocks.shape[0]
    return lax.dynamic_slice_in_dim(jnp.concatenate([blocks, blocks], 0), first, count, 0)


def reduce_scatter(piece, size, long_way, axis):
    half = size // 2
    ahead, back = ring(size, 1), ring(size, -1)
    f_len, b_len = (half, size - 1 - half) if long_way > 0 else (size - 1 - half, half)
    f = b = None
    for d in range(half, 0, -1):
        if d <= f_len:
            own = piece(d)
            f = lax.ppermute(own if f is None else (own.astype(f32) + f.astype(f32)).astype(bf16), axis, ahead)
        if d <= b_len:
            own = piece(-d)
            b = lax.ppermute(own if b is None else (own.astype(f32) + b.astype(f32)).astype(bf16), axis, back)
    return piece(0).astype(f32) + f.astype(f32) + b.astype(f32)


def all_gather(block, size, long_way, axis):
    half = size // 2
    ahead, back = ring(size, 1), ring(size, -1)
    f_len, b_len = (half, size - 1 - half) if long_way > 0 else (size - 1 - half, half)
    out = {0: block}
    f = b = block
    for d in range(1, half + 1):
        if d <= f_len:
            f = lax.ppermute(f, axis, ahead)
            out[size - d] = f
        if d <= b_len:
            b = lax.ppermute(b, axis, back)
            out[d] = b
    return [out[d] for d in range(size)]


def per_device(
    tokens,
    routes,
    route_weights,
    norm_gain,
    expert_gate,
    expert_up,
    expert_down,
    shared_gate,
    shared_up,
    shared_down,
    out_gain,
):
    tok_count, width = tokens.shape
    tp = lax.axis_size("tp")
    experts = lax.axis_size("ep")
    full_width = width * tp
    me_tp = lax.axis_index("tp")
    top_count = routes.shape[1]
    capacity = min(tok_count, 2 * tok_count * top_count // experts)
    gain = lax.dynamic_slice_in_dim(norm_gain, me_tp * width, width, 0)
    gate_matrix, up_matrix, down_matrix = expert_gate[0], expert_up[0], expert_down[0]
    hidden_units = gate_matrix.shape[1]

    expert_ids = lax.broadcasted_iota(jnp.int32, (1, 1, experts), 2)
    hit = routes[:, :, None] == expert_ids
    routed = jnp.any(hit, axis=1)
    weight = jnp.sum(jnp.where(hit, route_weights[:, :, None], 0.0), axis=1)
    lower = (
        lax.broadcasted_iota(jnp.int32, (tok_count, tok_count), 0)
        >= lax.broadcasted_iota(jnp.int32, (tok_count, tok_count), 1)
    ).astype(bf16)
    place = jnp.where(routed, dot(lower, routed.astype(bf16)) - 1.0, -1.0).astype(bf16)
    weight_high = weight.astype(bf16)
    weight_low = (weight - weight_high.astype(f32)).astype(bf16)

    def picking(first, count):
        columns = experts * count
        column = lax.broadcasted_iota(jnp.int32, (experts, columns), 1)
        expand = (column // count == lax.broadcasted_iota(jnp.int32, (experts, columns), 0)).astype(bf16)
        slot = (lax.broadcasted_iota(jnp.int32, (1, columns), 1) % count + first).astype(f32)
        pick = dot(place, expand) == slot
        high = jnp.where(pick, dot(weight_high, expand), 0.0).astype(bf16)
        low = jnp.where(pick, dot(weight_low, expand), 0.0).astype(bf16)
        return pick.astype(bf16), high, low

    def leaving(pick):
        rows = lax.dot_general(pick, tokens, (((0,), (0,)), ((), ())), preferred_element_type=f32)
        return rows.astype(bf16).reshape(experts, -1, width)

    def swapped(rows):
        return lax.all_to_all(rows, "ep", 0, 0, tiled=True)

    def partials(rows, gate, up):
        rows = rows.astype(f32)
        squares = jnp.sum(rows * rows, axis=1, keepdims=True)
        squares = jnp.broadcast_to(squares, (rows.shape[0], 128)).astype(bf16)
        scaled = (rows * gain).astype(bf16)
        both = jnp.concatenate([scaled, squares], 1)
        both = turned(both.reshape(tp, -1, both.shape[1]), me_tp).reshape(rows.shape[0], -1)
        scaled, squares = both[:, :width], both[:, width:]
        gate_part = dot(scaled, gate).astype(bf16)
        up_part = dot(scaled, up).astype(bf16)
        return [v.reshape(tp, -1, v.shape[1]) for v in (gate_part, up_part, squares)]

    def hidden_of(total):
        scale = lax.rsqrt(total[:, 2 * hidden_units : 2 * hidden_units + 1] / full_width + epsilon)
        gate_value = total[:, :hidden_units] * scale
        up_value = total[:, hidden_units : 2 * hidden_units] * scale
        return (jax.nn.silu(gate_value) * up_value).astype(bf16)

    def unturned(rows):
        return turned(rows.reshape(tp, -1, rows.shape[1]), (tp - me_tp) % tp).reshape(rows.shape)

    def returned(hidden, high, low):
        rows = unturned(dot(hidden, down_matrix).astype(bf16)).reshape(experts, -1, width)
        rows = lax.all_to_all(rows, "ep", 0, 0, tiled=True).reshape(-1, width)
        return dot(high, rows) + dot(low, rows)

    first_count = 5 * capacity // 8
    pick_a, high_a, low_a = picking(0, first_count)
    pick_b, high_b, low_b = picking(first_count, capacity - first_count)
    rows_a = swapped(leaving(pick_a))
    rows_b = leaving(pick_b)
    rows_a, rows_b = lax.optimization_barrier((rows_a, rows_b))
    rows_a = rows_a.reshape(-1, width)
    rows_b = swapped(rows_b).reshape(-1, width)

    parts_s = partials(tokens, shared_gate, shared_up)
    parts_a = partials(rows_a, gate_matrix, up_matrix)
    parts_b = partials(rows_b, gate_matrix, up_matrix)

    def piece_a(d):
        return jnp.concatenate([v[d % tp] for v in parts_a], 1)

    def piece_b(d):
        return jnp.concatenate(
            [jnp.concatenate([v[d % tp] for v in parts], 1) for parts in (parts_s, parts_b)], 0
        )

    hidden_a = hidden_of(reduce_scatter(piece_a, tp, -1, "tp"))
    hidden_b = hidden_of(reduce_scatter(piece_b, tp, 1, "tp"))
    all_a = jnp.concatenate(all_gather(hidden_a, tp, 1, "tp"), 0)
    all_b = all_gather(hidden_b, tp, -1, "tp")
    shared_rows = tok_count // tp
    all_s = jnp.concatenate([v[:shared_rows] for v in all_b], 0)
    all_b = jnp.concatenate([v[shared_rows:] for v in all_b], 0)

    mixture = returned(all_a, high_a, low_a) + unturned(dot(all_s, shared_down))
    mixture = mixture + returned(all_b, high_b, low_b)

    square_sum = jnp.sum(mixture * mixture, axis=-1, keepdims=True)
    copies = jnp.broadcast_to(square_sum[None], (tp, *square_sum.shape))
    square_sum = lax.all_to_all(copies, "tp", 0, 0, tiled=True).sum(axis=0)
    scale = lax.rsqrt(square_sum / full_width + epsilon)
    return (mixture * scale * out_gain).astype(bf16)


def solution(mesh):
    return jax.shard_map(
        per_device,
        mesh=mesh,
        in_specs=(
            P(("grp", "ep"), "tp"),
            P(("grp", "ep"), None),
            P(("grp", "ep"), None),
            P(),
            P("ep", "tp", None),
            P("ep", "tp", None),
            P("ep", None, "tp"),
            P("tp", None),
            P("tp", None),
            P(None, "tp"),
            P("tp"),
        ),
        out_specs=P(("grp", "ep"), "tp"),
        check_vma=False,
    )
```

```python
import jax
import jax.numpy as jnp
from jax import lax
from jax.experimental import pallas as pl
from jax.experimental.pallas import tpu as pltpu
from jax.sharding import PartitionSpec as P


epsilon = 1e-06
f32 = jnp.float32
bf16 = jnp.bfloat16


def dot(a, b):
    return jnp.dot(a, b, preferred_element_type=f32)


def ring(count, step):
    return [(i, (i + step) % count) for i in range(count)]


def added(own, came):
    return own if came is None else (own.astype(f32) + came.astype(f32)).astype(bf16)


def reduce_scatter(piece, size, long_way, axis, late=None):
    half = size // 2
    ahead, back = ring(size, 1), ring(size, -1)
    f_len, b_len = (half, size - 1 - half) if long_way > 0 else (size - 1 - half, half)
    f = b = None
    for d in range(half, 0, -1):
        if d <= f_len:
            f = added(piece[d], f)
        if d <= b_len:
            b = added(piece[size - d], b)
        if d == half - 1 and late is not None:
            f, b, late = lax.optimization_barrier((f, b, late))
        if d <= f_len:
            f = lax.ppermute(f, axis, ahead)
        if d <= b_len:
            b = lax.ppermute(b, axis, back)
    return piece[0].astype(f32) + f.astype(f32) + b.astype(f32), late


def all_gather(block, size, long_way, axis):
    half = size // 2
    ahead, back = ring(size, 1), ring(size, -1)
    f_len, b_len = (half, size - 1 - half) if long_way > 0 else (size - 1 - half, half)
    out = {0: block}
    f = b = block
    for d in range(1, half + 1):
        if d <= f_len:
            f = lax.ppermute(f, axis, ahead)
            out[size - d] = f
        if d <= b_len:
            b = lax.ppermute(b, axis, back)
            out[d] = b
    return [out[d] for d in range(size)]


LANES = 128
TILE = 256
IN_VMEM = pl.BlockSpec()
IN_SMEM = pl.BlockSpec(memory_space=pltpu.SMEM)


def block_row(me, d, size, rows):
    return pl.multiple_of(lax.rem(me + d, size) * rows, 16)


def project(me, gain, sources, size, space):
    counts = [rows.shape[0] // size for rows, _, _ in sources]
    width = sources[0][0].shape[1]
    units = sources[0][1].shape[1]
    height = sum(counts)

    def body(me_ref, gain_ref, *refs):
        ins, outs, scratch = refs[: 3 * len(counts)], refs[3 * len(counts) : 3 * len(counts) + size], refs[-len(counts) :]
        first = 0
        for i, count in enumerate(counts):
            rows_ref, gate_ref, up_ref = ins[3 * i : 3 * i + 3]
            turned_ref = scratch[i]
            for d in range(size):
                rows = rows_ref[pl.ds(block_row(me_ref[0], d, size, count), count), :].astype(f32)
                squares = jnp.sum(rows * rows, axis=1, keepdims=True)
                outs[d][first : first + count, 2 * units :] = jnp.broadcast_to(squares, (count, LANES)).astype(bf16)
                turned_ref[d * count : (d + 1) * count, :] = (rows * gain_ref[...]).astype(bf16)

            def columns(n, _, gate_ref=gate_ref, up_ref=up_ref, turned_ref=turned_ref, first=first, count=count):
                at = pl.multiple_of(n * TILE, TILE)
                for ref, base in ((gate_ref, 0), (up_ref, units)):
                    value = dot(turned_ref[...], ref[:, pl.ds(at, TILE)]).astype(bf16)
                    for d in range(size):
                        outs[d][first : first + count, pl.ds(pl.multiple_of(base + at, TILE), TILE)] = value[
                            d * count : (d + 1) * count
                        ]
                return 0

            lax.fori_loop(0, units // TILE, columns, 0)
            first += count

    return pl.pallas_call(
        body,
        out_shape=[space((height, 2 * units + LANES), bf16)] * size,
        in_specs=[IN_SMEM, IN_VMEM] + [IN_VMEM] * (3 * len(counts)),
        out_specs=[IN_VMEM] * size,
        scratch_shapes=[pltpu.VMEM((size * count, width), bf16) for count in counts],
        name="project",
        compiler_params=pltpu.CompilerParams(vmem_limit_bytes=16 << 20),
    )(me, gain, *[v for rows, gate, up in sources for v in (rows, gate, up)])


def lower_down(me, blocks, sinks):
    size = len(blocks)
    units = blocks[0].shape[1]
    counts = [count for count, _, _ in sinks]
    width = sinks[0][1].shape[1]

    def body(me_ref, *refs):
        ins, mats = refs[:size], refs[size : size + len(counts)]
        outs, scratch = refs[size + len(counts) : size + 2 * len(counts)], refs[size + 2 * len(counts) :]
        first = 0
        for i, count in enumerate(counts):
            for d in range(size):
                scratch[i][pl.ds(block_row(me_ref[0], d, size, count), count), :] = ins[d][first : first + count, :]

            def columns(n, _, i=i):
                at = pl.multiple_of(n * TILE, TILE)
                outs[i][:, pl.ds(at, TILE)] = dot(scratch[i][...], mats[i][:, pl.ds(at, TILE)]).astype(outs[i].dtype)
                return 0

            lax.fori_loop(0, width // TILE, columns, 0)
            first += count

    return pl.pallas_call(
        body,
        out_shape=[jax.ShapeDtypeStruct((size * count, width), kind) for count, _, kind in sinks],
        in_specs=[IN_SMEM] + [IN_VMEM] * (size + len(counts)),
        out_specs=[IN_VMEM] * len(counts),
        scratch_shapes=[pltpu.VMEM((size * count, units), bf16) for count in counts],
        name="lower_down",
        compiler_params=pltpu.CompilerParams(vmem_limit_bytes=12 << 20),
    )(me, *blocks, *[matrix for _, matrix, _ in sinks])


def layer(
    tokens,
    routes,
    route_weights,
    norm_gain,
    expert_gate,
    expert_up,
    expert_down,
    shared_gate,
    shared_up,
    shared_down,
    out_gain,
):
    tok_count, width = tokens.shape
    tp = lax.axis_size("tp")
    experts = lax.axis_size("ep")
    full_width = width * tp
    me_tp = lax.axis_index("tp")
    top_count = routes.shape[1]
    capacity = min(tok_count, 2 * tok_count * top_count // experts)
    gain = lax.dynamic_slice_in_dim(norm_gain, me_tp * width, width, 0)
    gate_matrix, up_matrix, down_matrix = expert_gate[0], expert_up[0], expert_down[0]
    hidden_units = gate_matrix.shape[1]

    expert_ids = lax.broadcasted_iota(jnp.int32, (1, 1, experts), 2)
    hit = routes[:, :, None] == expert_ids
    routed = jnp.any(hit, axis=1)
    weight = jnp.sum(jnp.where(hit, route_weights[:, :, None], 0.0), axis=1)
    lower = (
        lax.broadcasted_iota(jnp.int32, (tok_count, tok_count), 0)
        >= lax.broadcasted_iota(jnp.int32, (tok_count, tok_count), 1)
    ).astype(bf16)
    place = jnp.where(routed, dot(lower, routed.astype(bf16)) - 1.0, -1.0).astype(bf16)
    weight_high = weight.astype(bf16)
    weight_low = (weight - weight_high.astype(f32)).astype(bf16)

    def picking(first, count):
        columns = experts * count
        column = lax.broadcasted_iota(jnp.int32, (experts, columns), 1)
        expand = (column // count == lax.broadcasted_iota(jnp.int32, (experts, columns), 0)).astype(bf16)
        slot = (lax.broadcasted_iota(jnp.int32, (1, columns), 1) % count + first).astype(f32)
        pick = dot(place, expand) == slot
        high = jnp.where(pick, dot(weight_high, expand), 0.0).astype(bf16)
        low = jnp.where(pick, dot(weight_low, expand), 0.0).astype(bf16)
        return pick.astype(bf16), high, low

    def leaving(pick):
        rows = lax.dot_general(pick, tokens, (((0,), (0,)), ((), ())), preferred_element_type=f32)
        return rows.astype(bf16).reshape(experts, -1, width)

    def swapped(rows):
        return lax.all_to_all(rows, "ep", 0, 0, tiled=True)

    def hidden_of(total):
        scale = lax.rsqrt(total[:, 2 * hidden_units : 2 * hidden_units + 1] / full_width + epsilon)
        gate_value = total[:, :hidden_units] * scale
        up_value = total[:, hidden_units : 2 * hidden_units] * scale
        return (jax.nn.silu(gate_value) * up_value).astype(bf16)

    first_count = 5 * capacity // 8
    pick_a, high_a, low_a = picking(0, first_count)
    pick_b, high_b, low_b = picking(first_count, capacity - first_count)
    rows_a = swapped(leaving(pick_a))
    rows_b = leaving(pick_b)
    rows_a, rows_b = lax.optimization_barrier((rows_a, rows_b))
    rows_b = swapped(rows_b)
    me = me_tp.reshape(1)
    gain = gain[None]

    pieces_a = project(me, gain, [(rows_a.reshape(-1, width), gate_matrix, up_matrix)], tp, pltpu.HBM)
    total_a, rows_b = reduce_scatter(pieces_a, tp, -1, "tp", late=rows_b)
    pieces_b = project(
        me,
        gain,
        [(tokens, shared_gate, shared_up), (rows_b.reshape(-1, width), gate_matrix, up_matrix)],
        tp,
        jax.ShapeDtypeStruct,
    )
    total_b, _ = reduce_scatter(pieces_b, tp, 1, "tp")
    blocks_a = all_gather(hidden_of(total_a), tp, 1, "tp")
    blocks_b = all_gather(hidden_of(total_b), tp, -1, "tp")
    (down_a,) = lower_down(me, blocks_a, [(blocks_a[0].shape[0], down_matrix, bf16)])
    shared_rows = tok_count // tp
    shared_out, down_b = lower_down(
        me,
        blocks_b,
        [(shared_rows, shared_down, f32), (blocks_b[0].shape[0] - shared_rows, down_matrix, bf16)],
    )
    back_a = swapped(down_a.reshape(experts, -1, width))
    back_a, down_b = lax.optimization_barrier((back_a, down_b))
    back_b = swapped(down_b.reshape(experts, -1, width)).reshape(-1, width)
    back_a = back_a.reshape(-1, width)
    mixture = shared_out + dot(high_a, back_a) + dot(low_a, back_a) + dot(high_b, back_b) + dot(low_b, back_b)

    square_sum = jnp.sum(mixture * mixture, axis=-1, keepdims=True)
    copies = jnp.broadcast_to(square_sum[None], (tp, *square_sum.shape))
    square_sum = lax.all_to_all(copies, "tp", 0, 0, tiled=True).sum(axis=0)
    scale = lax.rsqrt(square_sum / full_width + epsilon)
    return (mixture * scale * out_gain).astype(bf16)


def solution(mesh):
    return jax.shard_map(
        layer,
        mesh=mesh,
        in_specs=(
            P(("grp", "ep"), "tp"),
            P(("grp", "ep"), None),
            P(("grp", "ep"), None),
            P(),
            P("ep", "tp", None),
            P("ep", "tp", None),
            P("ep", None, "tp"),
            P("tp", None),
            P("tp", None),
            P(None, "tp"),
            P("tp"),
        ),
        out_specs=P(("grp", "ep"), "tp"),
        check_vma=False,
    )
```

```python
import jax
import jax.numpy as jnp
from jax import lax
from jax.experimental import pallas as pl
from jax.experimental.pallas import tpu as pltpu
from jax.sharding import PartitionSpec as P


epsilon = 1e-06
f32 = jnp.float32
bf16 = jnp.bfloat16


def dot(a, b):
    return jnp.dot(a, b, preferred_element_type=f32)


def ring(count, step):
    return [(i, (i + step) % count) for i in range(count)]


def added(own, came):
    return own if came is None else (own.astype(f32) + came.astype(f32)).astype(bf16)


def reduce_scatter(piece, size, long_way, axis):
    half = size // 2
    ahead, back = ring(size, 1), ring(size, -1)
    f_len, b_len = (half, size - 1 - half) if long_way > 0 else (size - 1 - half, half)
    f = b = None
    for d in range(half, 0, -1):
        if d <= f_len:
            f = lax.ppermute(added(piece[d], f), axis, ahead)
        if d <= b_len:
            b = lax.ppermute(added(piece[size - d], b), axis, back)
    return piece[0].astype(f32) + f.astype(f32) + b.astype(f32)


def all_gather(block, size, long_way, axis):
    half = size // 2
    ahead, back = ring(size, 1), ring(size, -1)
    f_len, b_len = (half, size - 1 - half) if long_way > 0 else (size - 1 - half, half)
    out = {0: block}
    f = b = block
    for d in range(1, half + 1):
        if d <= f_len:
            f = lax.ppermute(f, axis, ahead)
            out[size - d] = f
        if d <= b_len:
            b = lax.ppermute(b, axis, back)
            out[d] = b
    return [out[d] for d in range(size)]


LANES = 128
TILE = 256
IN_VMEM = pl.BlockSpec()
IN_SMEM = pl.BlockSpec(memory_space=pltpu.SMEM)


def block_row(me, d, size, rows):
    return pl.multiple_of(lax.rem(me + d, size) * rows, 16)


def project(me, gain, rows, gate, up, size, streams):
    height, width = rows.shape
    units = gate.shape[1]
    part = height // streams
    count = part // size

    def body(me_ref, gain_ref, rows_ref, gate_ref, up_ref, *refs):
        outs, turned_ref = refs[:-1], refs[-1]
        for k in range(streams * size):
            at = pl.multiple_of(k // size * part + block_row(me_ref[0], k % size, size, count), 16)
            block = rows_ref[pl.ds(at, count), :].astype(f32)
            squares = jnp.sum(block * block, axis=1, keepdims=True)
            outs[k][:, 2 * units :] = jnp.broadcast_to(squares, (count, LANES)).astype(bf16)
            turned_ref[k * count : (k + 1) * count, :] = (block * gain_ref[...]).astype(bf16)

        def columns(n, _):
            at = pl.multiple_of(n * TILE, TILE)
            for ref, base in ((gate_ref, 0), (up_ref, units)):
                value = dot(turned_ref[...], ref[:, pl.ds(at, TILE)]).astype(bf16)
                for k in range(streams * size):
                    outs[k][:, pl.ds(pl.multiple_of(base + at, TILE), TILE)] = value[k * count : (k + 1) * count]
            return 0

        lax.fori_loop(0, units // TILE, columns, 0)

    out = pl.pallas_call(
        body,
        out_shape=[jax.ShapeDtypeStruct((count, 2 * units + LANES), bf16)] * (streams * size),
        in_specs=[IN_SMEM] + [IN_VMEM] * 4,
        out_specs=[IN_VMEM] * (streams * size),
        scratch_shapes=[pltpu.VMEM((height, width), bf16)],
        compiler_params=pltpu.CompilerParams(vmem_limit_bytes=16 << 20),
        name="project",
    )(me, gain, rows, gate, up)
    return [out[k * size : (k + 1) * size] for k in range(streams)]


def lower_down(me, blocks_a, blocks_b, matrix, shared_matrix):
    size = len(blocks_a)
    count, units = blocks_a[0].shape
    shared = blocks_b[0].shape[0] - count
    width = matrix.shape[1]
    part = size * count

    def body(me_ref, *refs):
        ins_a, ins_b = refs[:size], refs[size : 2 * size]
        matrix_ref, shared_ref, out_ref, shared_out_ref, rows_ref, shared_rows_ref = refs[2 * size :]
        for d in range(size):
            at = block_row(me_ref[0], d, size, count)
            rows_ref[pl.ds(at, count), :] = ins_a[d][...]
            rows_ref[pl.ds(pl.multiple_of(part + at, 16), count), :] = ins_b[d][:count, :]
            shared_rows_ref[pl.ds(block_row(me_ref[0], d, size, shared), shared), :] = ins_b[d][count:, :]

        def columns(n, _):
            at = pl.multiple_of(n * TILE, TILE)
            out_ref[:, pl.ds(at, TILE)] = dot(rows_ref[...], matrix_ref[:, pl.ds(at, TILE)]).astype(bf16)
            shared_out_ref[:, pl.ds(at, TILE)] = dot(shared_rows_ref[...], shared_ref[:, pl.ds(at, TILE)])
            return 0

        lax.fori_loop(0, width // TILE, columns, 0)

    return pl.pallas_call(
        body,
        out_shape=[jax.ShapeDtypeStruct((2 * part, width), bf16), jax.ShapeDtypeStruct((size * shared, width), f32)],
        in_specs=[IN_SMEM] + [IN_VMEM] * (2 * size + 2),
        out_specs=[IN_VMEM] * 2,
        scratch_shapes=[pltpu.VMEM((2 * part, units), bf16), pltpu.VMEM((size * shared, units), bf16)],
        compiler_params=pltpu.CompilerParams(vmem_limit_bytes=14 << 20),
        name="lower_down",
    )(me, *blocks_a, *blocks_b, matrix, shared_matrix)


def layer(
    tokens,
    routes,
    route_weights,
    norm_gain,
    expert_gate,
    expert_up,
    expert_down,
    shared_gate,
    shared_up,
    shared_down,
    out_gain,
):
    tok_count, width = tokens.shape
    tp = lax.axis_size("tp")
    experts = lax.axis_size("ep")
    full_width = width * tp
    me_tp = lax.axis_index("tp")
    top_count = routes.shape[1]
    capacity = min(tok_count, 2 * tok_count * top_count // experts)
    gain = lax.dynamic_slice_in_dim(norm_gain, me_tp * width, width, 0)
    gate_matrix, up_matrix, down_matrix = expert_gate[0], expert_up[0], expert_down[0]
    hidden_units = gate_matrix.shape[1]

    expert_ids = lax.broadcasted_iota(jnp.int32, (1, 1, experts), 2)
    hit = routes[:, :, None] == expert_ids
    routed = jnp.any(hit, axis=1)
    weight = jnp.sum(jnp.where(hit, route_weights[:, :, None], 0.0), axis=1)
    lower = (
        lax.broadcasted_iota(jnp.int32, (tok_count, tok_count), 0)
        >= lax.broadcasted_iota(jnp.int32, (tok_count, tok_count), 1)
    ).astype(bf16)
    place = jnp.where(routed, dot(lower, routed.astype(bf16)) - 1.0, -1.0).astype(bf16)
    weight_high = weight.astype(bf16)
    weight_low = (weight - weight_high.astype(f32)).astype(bf16)

    columns = experts * capacity
    column = lax.broadcasted_iota(jnp.int32, (experts, columns), 1)
    expand = (column // capacity == lax.broadcasted_iota(jnp.int32, (experts, columns), 0)).astype(bf16)
    slot = (lax.broadcasted_iota(jnp.int32, (1, columns), 1) % capacity).astype(f32)
    pick = dot(place, expand) == slot
    high = jnp.where(pick, dot(weight_high, expand), 0.0).astype(bf16)
    low = jnp.where(pick, dot(weight_low, expand), 0.0).astype(bf16)

    def swapped(rows):
        return lax.all_to_all(rows.reshape(experts, capacity, width), "ep", 0, 0, tiled=True).reshape(columns, width)

    def hidden_of(total):
        scale = lax.rsqrt(total[:, 2 * hidden_units : 2 * hidden_units + 1] / full_width + epsilon)
        gate_value = total[:, :hidden_units] * scale
        up_value = total[:, hidden_units : 2 * hidden_units] * scale
        return (jax.nn.silu(gate_value) * up_value).astype(bf16)

    me = me_tp.reshape(1)
    gain = gain[None]
    leaving = lax.dot_general(pick.astype(bf16), tokens, (((0,), (0,)), ((), ())), preferred_element_type=f32)
    rows = swapped(leaving.astype(bf16))

    (pieces_s,) = project(me, gain, tokens, shared_gate, shared_up, tp, 1)
    hidden_s = hidden_of(reduce_scatter(pieces_s, tp, 1, "tp"))
    rows, hidden_s = lax.optimization_barrier((rows, hidden_s))

    pieces_a, pieces_b = project(me, gain, rows, gate_matrix, up_matrix, tp, 2)
    total_a = reduce_scatter(pieces_a, tp, -1, "tp")
    total_b = reduce_scatter(pieces_b, tp, 1, "tp")
    blocks_a = all_gather(hidden_of(total_a), tp, 1, "tp")
    blocks_b = all_gather(jnp.concatenate([hidden_of(total_b), hidden_s], 0), tp, -1, "tp")
    down, shared_out = lower_down(me, blocks_a, blocks_b, down_matrix, shared_down)
    came = swapped(down)
    mixture = shared_out + dot(high, came) + dot(low, came)

    square_sum = jnp.sum(mixture * mixture, axis=-1, keepdims=True)
    copies = jnp.broadcast_to(square_sum[None], (tp, *square_sum.shape))
    square_sum = lax.all_to_all(copies, "tp", 0, 0, tiled=True).sum(axis=0)
    scale = lax.rsqrt(square_sum / full_width + epsilon)
    return (mixture * scale * out_gain).astype(bf16)


def solution(mesh):
    return jax.shard_map(
        layer,
        mesh=mesh,
        in_specs=(
            P(("grp", "ep"), "tp"),
            P(("grp", "ep"), None),
            P(("grp", "ep"), None),
            P(),
            P("ep", "tp", None),
            P("ep", "tp", None),
            P("ep", None, "tp"),
            P("tp", None),
            P("tp", None),
            P(None, "tp"),
            P("tp"),
        ),
        out_specs=P(("grp", "ep"), "tp"),
        check_vma=False,
    )
```

```python
import jax
import jax.numpy as jnp
from jax import lax
from jax.experimental import pallas as pl
from jax.experimental.pallas import tpu as pltpu
from jax.sharding import PartitionSpec as P


epsilon = 1e-06
f32 = jnp.float32
bf16 = jnp.bfloat16


def dot(a, b):
    return jnp.dot(a, b, preferred_element_type=f32)


def ring(count, step):
    return [(i, (i + step) % count) for i in range(count)]


def added(own, came):
    return own if came is None else (own.astype(f32) + came.astype(f32)).astype(bf16)


def held(values, waited):
    if not waited:
        return values
    return lax.optimization_barrier((tuple(values), tuple(waited)))[0]


class Stream:
    def __init__(self, pieces, size, axis, long_way):
        self.pieces, self.size, self.axis = pieces, size, axis
        self.ways = (ring(size, 1), ring(size, -1))
        half = size // 2
        self.lengths = (half, size - 1 - half) if long_way > 0 else (size - 1 - half, half)
        self.came = [None, None]

    def sent(self, values, waited):
        came = [None, None]
        for i in (0, 1):
            if values[i] is not None:
                value = values[i] if waited[i] is None else held([values[i]], [waited[i]])[0]
                came[i] = self.came[i] = lax.ppermute(value, self.axis, self.ways[i])
        return came

    def scatter(self, step, waited):
        d = self.size // 2 - step
        places = (d, self.size - d)
        values = [added(self.pieces[places[i]], self.came[i]) if d <= self.lengths[i] else None for i in (0, 1)]
        return self.sent(values, waited)

    def total(self):
        return sum((v.astype(f32) for v in self.came), self.pieces[0].astype(f32))

    def open(self, block):
        self.blocks = {0: block}
        self.came = [block, block]
        self.lengths = self.lengths[::-1]

    def gather(self, step, waited):
        d = step + 1
        came = self.sent([self.came[i] if d <= self.lengths[i] else None for i in (0, 1)], waited)
        for i, place in ((0, self.size - d), (1, d)):
            if d <= self.lengths[i]:
                self.blocks[place] = self.came[i]
        return came

    def gathered(self):
        return [self.blocks[d] for d in range(self.size)]


LANES = 128
TILE = 256
IN_VMEM = pl.BlockSpec()
IN_SMEM = pl.BlockSpec(memory_space=pltpu.SMEM)


def block_row(me, d, size, rows):
    return pl.multiple_of(lax.rem(me + d, size) * rows, 16)


def project(me, gain, rows, gate, up, size, space):
    height, width = rows.shape
    units = gate.shape[1]
    count = height // size

    def body(me_ref, gain_ref, rows_ref, gate_ref, up_ref, *refs):
        outs, turned_ref = refs[:-1], refs[-1]
        for d in range(size):
            block = rows_ref[pl.ds(block_row(me_ref[0], d, size, count), count), :].astype(f32)
            squares = jnp.sum(block * block, axis=1, keepdims=True)
            outs[d][:, 2 * units :] = jnp.broadcast_to(squares, (count, LANES)).astype(bf16)
            turned_ref[d * count : (d + 1) * count, :] = (block * gain_ref[...]).astype(bf16)

        def columns(n, _):
            at = pl.multiple_of(n * TILE, TILE)
            for ref, base in ((gate_ref, 0), (up_ref, units)):
                value = dot(turned_ref[...], ref[:, pl.ds(at, TILE)]).astype(bf16)
                for d in range(size):
                    outs[d][:, pl.ds(pl.multiple_of(base + at, TILE), TILE)] = value[d * count : (d + 1) * count]
            return 0

        lax.fori_loop(0, units // TILE, columns, 0)

    return pl.pallas_call(
        body,
        out_shape=[space((count, 2 * units + LANES), bf16)] * size,
        in_specs=[IN_SMEM] + [IN_VMEM] * 4,
        out_specs=[IN_VMEM] * size,
        scratch_shapes=[pltpu.VMEM((height, width), bf16)],
        compiler_params=pltpu.CompilerParams(vmem_limit_bytes=12 << 20),
        name="project",
    )(me, gain, rows, gate, up)


def lower_down(me, blocks, sinks):
    size = len(blocks)
    units = blocks[0].shape[1]
    counts = [count for count, _, _ in sinks]
    width = sinks[0][1].shape[1]

    def body(me_ref, *refs):
        ins, mats = refs[:size], refs[size : size + len(counts)]
        outs, scratch = refs[size + len(counts) : size + 2 * len(counts)], refs[size + 2 * len(counts) :]
        first = 0
        for i, count in enumerate(counts):
            for d in range(size):
                scratch[i][pl.ds(block_row(me_ref[0], d, size, count), count), :] = ins[d][first : first + count, :]

            def columns(n, _, i=i):
                at = pl.multiple_of(n * TILE, TILE)
                outs[i][:, pl.ds(at, TILE)] = dot(scratch[i][...], mats[i][:, pl.ds(at, TILE)]).astype(outs[i].dtype)
                return 0

            lax.fori_loop(0, width // TILE, columns, 0)
            first += count

    return pl.pallas_call(
        body,
        out_shape=[jax.ShapeDtypeStruct((size * count, width), kind) for count, _, kind in sinks],
        in_specs=[IN_SMEM] + [IN_VMEM] * (size + len(counts)),
        out_specs=[IN_VMEM] * len(counts),
        scratch_shapes=[pltpu.VMEM((size * count, units), bf16) for count in counts],
        compiler_params=pltpu.CompilerParams(vmem_limit_bytes=12 << 20),
        name="lower_down",
    )(me, *blocks, *[matrix for _, matrix, _ in sinks])


def layer(
    tokens,
    routes,
    route_weights,
    norm_gain,
    expert_gate,
    expert_up,
    expert_down,
    shared_gate,
    shared_up,
    shared_down,
    out_gain,
):
    tok_count, width = tokens.shape
    tp = lax.axis_size("tp")
    experts = lax.axis_size("ep")
    full_width = width * tp
    me_tp = lax.axis_index("tp")
    top_count = routes.shape[1]
    capacity = min(tok_count, 2 * tok_count * top_count // experts)
    gain = lax.dynamic_slice_in_dim(norm_gain, me_tp * width, width, 0)
    gate_matrix, up_matrix, down_matrix = expert_gate[0], expert_up[0], expert_down[0]
    hidden_units = gate_matrix.shape[1]

    expert_ids = lax.broadcasted_iota(jnp.int32, (1, 1, experts), 2)
    hit = routes[:, :, None] == expert_ids
    routed = jnp.any(hit, axis=1)
    weight = jnp.sum(jnp.where(hit, route_weights[:, :, None], 0.0), axis=1)
    lower = (
        lax.broadcasted_iota(jnp.int32, (tok_count, tok_count), 0)
        >= lax.broadcasted_iota(jnp.int32, (tok_count, tok_count), 1)
    ).astype(bf16)
    place = jnp.where(routed, dot(lower, routed.astype(bf16)) - 1.0, -1.0).astype(bf16)
    weight_high = weight.astype(bf16)
    weight_low = (weight - weight_high.astype(f32)).astype(bf16)

    part = capacity // 2
    columns = experts * part
    column = lax.broadcasted_iota(jnp.int32, (experts, 2 * columns), 1)
    expand = (column % columns // part == lax.broadcasted_iota(jnp.int32, (experts, 2 * columns), 0)).astype(bf16)
    column = lax.broadcasted_iota(jnp.int32, (1, 2 * columns), 1)
    slot = (column // columns * part + column % part).astype(f32)
    pick = dot(place, expand) == slot
    high = jnp.where(pick, dot(weight_high, expand), 0.0).astype(bf16)
    low = jnp.where(pick, dot(weight_low, expand), 0.0).astype(bf16)

    def swapped(rows):
        return lax.all_to_all(rows.reshape(experts, part, width), "ep", 0, 0, tiled=True).reshape(columns, width)

    def hidden_of(total):
        scale = lax.rsqrt(total[:, 2 * hidden_units : 2 * hidden_units + 1] / full_width + epsilon)
        gate_value = total[:, :hidden_units] * scale
        up_value = total[:, hidden_units : 2 * hidden_units] * scale
        return (jax.nn.silu(gate_value) * up_value).astype(bf16)

    me = me_tp.reshape(1)
    gain = gain[None]
    leaving = lax.dot_general(pick.astype(bf16), tokens, (((0,), (0,)), ((), ())), preferred_element_type=f32)
    leaving = leaving.astype(bf16)
    rows_a = swapped(leaving[:columns])
    (leaving_b,) = held([leaving[columns:]], [rows_a])
    rows_b = swapped(leaving_b)

    steps = tp // 2
    shared = Stream(project(me, gain, tokens, shared_gate, shared_up, tp, jax.ShapeDtypeStruct), tp, "tp", 1)
    for step in range(steps):
        shared.scatter(step, [None, None])
    hidden_s = hidden_of(shared.total())

    a = Stream(project(me, gain, rows_a, gate_matrix, up_matrix, tp, pltpu.HBM), tp, "tp", -1)
    b = Stream(project(me, gain, rows_b, gate_matrix, up_matrix, tp, jax.ShapeDtypeStruct), tp, "tp", 1)

    done = {id(a): 0, id(b): 0}
    came = []
    for stream in [a] + [a, b] * (2 * steps - 1) + [b]:
        step = done[id(stream)]
        done[id(stream)] += 1
        waited = came[-3] if len(came) > 2 else [None, None]
        if step < steps:
            came.append(stream.scatter(step, waited))
            continue
        if step == steps:
            hidden = hidden_of(stream.total())
            stream.open(jnp.concatenate([hidden, hidden_s], 0) if stream is a else hidden)
        came.append(stream.gather(step - steps, waited))

    shared_rows = tok_count // tp
    blocks_a, blocks_b = a.gathered(), b.gathered()
    down_a, shared_out = lower_down(
        me,
        blocks_a,
        [(blocks_b[0].shape[0], down_matrix, bf16), (shared_rows, shared_down, f32)],
    )
    back_a = swapped(down_a)
    (down_b,) = lower_down(me, blocks_b, [(blocks_b[0].shape[0], down_matrix, bf16)])
    (down_b,) = held([down_b], [back_a])
    back_b = swapped(down_b)
    mixture = shared_out + dot(high[:, :columns], back_a) + dot(low[:, :columns], back_a)
    mixture = mixture + dot(high[:, columns:], back_b) + dot(low[:, columns:], back_b)

    square_sum = jnp.sum(mixture * mixture, axis=-1, keepdims=True)
    copies = jnp.broadcast_to(square_sum[None], (tp, *square_sum.shape))
    square_sum = lax.all_to_all(copies, "tp", 0, 0, tiled=True).sum(axis=0)
    scale = lax.rsqrt(square_sum / full_width + epsilon)
    return (mixture * scale * out_gain).astype(bf16)


def solution(mesh):
    return jax.shard_map(
        layer,
        mesh=mesh,
        in_specs=(
            P(("grp", "ep"), "tp"),
            P(("grp", "ep"), None),
            P(("grp", "ep"), None),
            P(),
            P("ep", "tp", None),
            P("ep", "tp", None),
            P("ep", None, "tp"),
            P("tp", None),
            P("tp", None),
            P(None, "tp"),
            P("tp"),
        ),
        out_specs=P(("grp", "ep"), "tp"),
        check_vma=False,
    )
```

```python
import jax
import jax.numpy as jnp
from jax import lax
from jax.experimental import pallas as pl
from jax.experimental.pallas import tpu as pltpu
from jax.sharding import PartitionSpec as P


epsilon = 1e-06
f32 = jnp.float32
bf16 = jnp.bfloat16


def dot(a, b):
    return jnp.dot(a, b, preferred_element_type=f32)


def exchanges(size, flip):
    pairs = [[(i, (i + (1 if i % 2 == way else -1)) % size) for i in range(size)] for way in (0, 1)]
    return pairs[::-1] if flip else pairs


def added(own, came):
    return (own.astype(f32) + came.astype(f32)).astype(bf16)


def reduce_scatter(piece, size, flip, axis):
    one, two = exchanges(size, flip)
    half = size // 2
    x = lax.ppermute(piece[half], axis, one)
    y = None
    for d in range(half - 1, 0, -1):
        x, y = (
            lax.ppermute(added(piece[size - d], x), axis, two),
            lax.ppermute(piece[d] if y is None else added(piece[d], y), axis, one),
        )
        x, y = y, x
    return piece[0].astype(f32) + x.astype(f32) + y.astype(f32)


def all_gather(block, size, flip, axis):
    one, two = exchanges(size, flip)
    out = {0: block}
    x = y = block
    for d in range(1, size // 2):
        x, y = lax.ppermute(y, axis, one), lax.ppermute(x, axis, two)
        out[d], out[size - d] = x, y
    out[size // 2] = lax.ppermute(y, axis, one)
    return [out[d] for d in range(size)]


LANES = 128
TILE = 256
IN_VMEM = pl.BlockSpec()
IN_SMEM = pl.BlockSpec(memory_space=pltpu.SMEM)


def block_row(me, d, size, rows, flip):
    along = 1 - 2 * lax.rem(me, 2)
    return pl.multiple_of(lax.rem(me + size + (-d if flip else d) * along, size) * rows, 16)


def project(me, gain, rows, first, height, gate, up, size, flip):
    width = rows.shape[1]
    units = gate.shape[1]
    count = height // size

    def body(me_ref, gain_ref, rows_ref, gate_ref, up_ref, *refs):
        outs, turned_ref = refs[:-1], refs[-1]
        for d in range(size):
            at = pl.multiple_of(first + block_row(me_ref[0], d, size, count, flip), 16)
            block = rows_ref[pl.ds(at, count), :].astype(f32)
            squares = jnp.sum(block * block, axis=1, keepdims=True)
            outs[d][:, 2 * units :] = jnp.broadcast_to(squares, (count, LANES)).astype(bf16)
            turned_ref[d * count : (d + 1) * count, :] = (block * gain_ref[...]).astype(bf16)

        def columns(n, _):
            at = pl.multiple_of(n * TILE, TILE)
            for ref, base in ((gate_ref, 0), (up_ref, units)):
                value = dot(turned_ref[...], ref[:, pl.ds(at, TILE)]).astype(bf16)
                for d in range(size):
                    outs[d][:, pl.ds(pl.multiple_of(base + at, TILE), TILE)] = value[d * count : (d + 1) * count]
            return 0

        lax.fori_loop(0, units // TILE, columns, 0)

    return pl.pallas_call(
        body,
        out_shape=[jax.ShapeDtypeStruct((count, 2 * units + LANES), bf16)] * size,
        in_specs=[IN_SMEM] + [IN_VMEM] * 4,
        out_specs=[IN_VMEM] * size,
        scratch_shapes=[pltpu.VMEM((height, width), bf16)],
        compiler_params=pltpu.CompilerParams(vmem_limit_bytes=12 << 20),
        name="project",
    )(me, gain, rows, gate, up)


def lower_down(me, blocks_a, blocks_b, matrix, shared_matrix):
    size = len(blocks_a)
    count, units = blocks_a[0].shape
    shared = blocks_b[0].shape[0] - count
    width = matrix.shape[1]
    part = size * count

    def body(me_ref, *refs):
        ins_a, ins_b = refs[:size], refs[size : 2 * size]
        matrix_ref, shared_ref, out_ref, shared_out_ref, rows_ref, shared_rows_ref = refs[2 * size :]
        for d in range(size):
            at_a = block_row(me_ref[0], d, size, count, False)
            at_b = pl.multiple_of(part + block_row(me_ref[0], d, size, count, True), 16)
            at_s = block_row(me_ref[0], d, size, shared, True)
            rows_ref[pl.ds(at_a, count), :] = ins_a[d][...]
            rows_ref[pl.ds(at_b, count), :] = ins_b[d][:count, :]
            shared_rows_ref[pl.ds(at_s, shared), :] = ins_b[d][count:, :]

        def columns(n, _):
            at = pl.multiple_of(n * TILE, TILE)
            out_ref[:, pl.ds(at, TILE)] = dot(rows_ref[...], matrix_ref[:, pl.ds(at, TILE)]).astype(bf16)
            shared_out_ref[:, pl.ds(at, TILE)] = dot(shared_rows_ref[...], shared_ref[:, pl.ds(at, TILE)])
            return 0

        lax.fori_loop(0, width // TILE, columns, 0)

    return pl.pallas_call(
        body,
        out_shape=[jax.ShapeDtypeStruct((2 * part, width), bf16), jax.ShapeDtypeStruct((size * shared, width), f32)],
        in_specs=[IN_SMEM] + [IN_VMEM] * (2 * size + 2),
        out_specs=[IN_VMEM] * 2,
        scratch_shapes=[pltpu.VMEM((2 * part, units), bf16), pltpu.VMEM((size * shared, units), bf16)],
        compiler_params=pltpu.CompilerParams(vmem_limit_bytes=14 << 20),
        name="lower_down",
    )(me, *blocks_a, *blocks_b, matrix, shared_matrix)


def layer(
    tokens,
    routes,
    route_weights,
    norm_gain,
    expert_gate,
    expert_up,
    expert_down,
    shared_gate,
    shared_up,
    shared_down,
    out_gain,
):
    tok_count, width = tokens.shape
    tp = lax.axis_size("tp")
    experts = lax.axis_size("ep")
    full_width = width * tp
    me_tp = lax.axis_index("tp")
    top_count = routes.shape[1]
    capacity = min(tok_count, 2 * tok_count * top_count // experts)
    gain = lax.dynamic_slice_in_dim(norm_gain, me_tp * width, width, 0)
    gate_matrix, up_matrix, down_matrix = expert_gate[0], expert_up[0], expert_down[0]
    hidden_units = gate_matrix.shape[1]

    expert_ids = lax.broadcasted_iota(jnp.int32, (1, 1, experts), 2)
    hit = routes[:, :, None] == expert_ids
    routed = jnp.any(hit, axis=1)
    weight = jnp.sum(jnp.where(hit, route_weights[:, :, None], 0.0), axis=1)
    lower = (
        lax.broadcasted_iota(jnp.int32, (tok_count, tok_count), 0)
        >= lax.broadcasted_iota(jnp.int32, (tok_count, tok_count), 1)
    ).astype(bf16)
    place = jnp.where(routed, dot(lower, routed.astype(bf16)) - 1.0, -1.0).astype(bf16)
    weight_high = weight.astype(bf16)
    weight_low = (weight - weight_high.astype(f32)).astype(bf16)

    columns = experts * capacity
    column = lax.broadcasted_iota(jnp.int32, (experts, columns), 1)
    expand = (column // capacity == lax.broadcasted_iota(jnp.int32, (experts, columns), 0)).astype(bf16)
    slot = (lax.broadcasted_iota(jnp.int32, (1, columns), 1) % capacity).astype(f32)
    pick = dot(place, expand) == slot
    high = jnp.where(pick, dot(weight_high, expand), 0.0).astype(bf16)
    low = jnp.where(pick, dot(weight_low, expand), 0.0).astype(bf16)

    def swapped(rows):
        return lax.all_to_all(rows.reshape(experts, capacity, width), "ep", 0, 0, tiled=True).reshape(columns, width)

    def hidden_of(total):
        scale = lax.rsqrt(total[:, 2 * hidden_units : 2 * hidden_units + 1] / full_width + epsilon)
        gate_value = total[:, :hidden_units] * scale
        up_value = total[:, hidden_units : 2 * hidden_units] * scale
        return (jax.nn.silu(gate_value) * up_value).astype(bf16)

    me = me_tp.reshape(1)
    gain = gain[None]
    leaving = lax.dot_general(pick.astype(bf16), tokens, (((0,), (0,)), ((), ())), preferred_element_type=f32)
    rows = swapped(leaving.astype(bf16))

    pieces_s = project(me, gain, tokens, 0, tok_count, shared_gate, shared_up, tp, False)
    hidden_s = hidden_of(reduce_scatter(pieces_s, tp, False, "tp"))
    rows, hidden_s = lax.optimization_barrier((rows, hidden_s))

    part = columns // 2
    pieces_a = project(me, gain, rows, 0, part, gate_matrix, up_matrix, tp, False)
    pieces_b = project(me, gain, rows, part, part, gate_matrix, up_matrix, tp, True)
    total_a = reduce_scatter(pieces_a, tp, False, "tp")
    total_b = reduce_scatter(pieces_b, tp, True, "tp")
    blocks_a = all_gather(hidden_of(total_a), tp, False, "tp")
    blocks_b = all_gather(jnp.concatenate([hidden_of(total_b), hidden_s], 0), tp, True, "tp")
    down, shared_out = lower_down(me, blocks_a, blocks_b, down_matrix, shared_down)
    came = swapped(down)
    mixture = shared_out + dot(high, came) + dot(low, came)

    square_sum = jnp.sum(mixture * mixture, axis=-1, keepdims=True)
    copies = jnp.broadcast_to(square_sum[None], (tp, *square_sum.shape))
    square_sum = lax.all_to_all(copies, "tp", 0, 0, tiled=True).sum(axis=0)
    scale = lax.rsqrt(square_sum / full_width + epsilon)
    return (mixture * scale * out_gain).astype(bf16)


def solution(mesh):
    return jax.shard_map(
        layer,
        mesh=mesh,
        in_specs=(
            P(("grp", "ep"), "tp"),
            P(("grp", "ep"), None),
            P(("grp", "ep"), None),
            P(),
            P("ep", "tp", None),
            P("ep", "tp", None),
            P("ep", None, "tp"),
            P("tp", None),
            P("tp", None),
            P(None, "tp"),
            P("tp"),
        ),
        out_specs=P(("grp", "ep"), "tp"),
        check_vma=False,
    )
```

```python
import jax
import jax.numpy as jnp
from jax import lax
from jax.experimental import pallas as pl
from jax.experimental.pallas import tpu as pltpu
from jax.sharding import PartitionSpec as P


epsilon = 1e-06
f32 = jnp.float32
bf16 = jnp.bfloat16


def dot(a, b):
    return jnp.dot(a, b, preferred_element_type=f32)


def exchanges(size, flip):
    pairs = [[(i, (i + (1 if i % 2 == way else -1)) % size) for i in range(size)] for way in (0, 1)]
    return pairs[::-1] if flip else pairs


def added(own, came):
    return (own.astype(f32) + came.astype(f32)).astype(bf16)


def reduce_scatter(piece, size, flip, axis):
    one, two = exchanges(size, flip)
    half = size // 2
    x = lax.ppermute(piece[half], axis, one)
    y = None
    for d in range(half - 1, 0, -1):
        x, y = (
            lax.ppermute(added(piece[size - d], x), axis, two),
            lax.ppermute(piece[d] if y is None else added(piece[d], y), axis, one),
        )
        x, y = y, x
    return piece[0].astype(f32) + x.astype(f32) + y.astype(f32)


def all_gather(block, size, flip, axis):
    one, two = exchanges(size, flip)
    out = {0: block}
    x = y = block
    for d in range(1, size // 2):
        x, y = lax.ppermute(y, axis, one), lax.ppermute(x, axis, two)
        out[d], out[size - d] = x, y
    out[size // 2] = lax.ppermute(y, axis, one)
    return [out[d] for d in range(size)]


LANES = 128
TILE = 256
STREAMS = 3
IN_VMEM = pl.BlockSpec()
IN_SMEM = pl.BlockSpec(memory_space=pltpu.SMEM)


def block_row(me, d, size, rows, flip):
    along = 1 - 2 * lax.rem(me, 2)
    return pl.multiple_of(lax.rem(me + size + (-d if flip else d) * along, size) * rows, 16)


def project(me, gain, rows, first, height, gate, up, size, flip):
    width = rows.shape[1]
    units = gate.shape[1]
    count = height // size

    def body(me_ref, gain_ref, rows_ref, gate_ref, up_ref, *refs):
        outs, turned_ref = refs[:-1], refs[-1]
        for d in range(size):
            at = pl.multiple_of(first + block_row(me_ref[0], d, size, count, flip), 16)
            block = rows_ref[pl.ds(at, count), :].astype(f32)
            squares = jnp.sum(block * block, axis=1, keepdims=True)
            outs[d][:, 2 * units :] = jnp.broadcast_to(squares, (count, LANES)).astype(bf16)
            turned_ref[d * count : (d + 1) * count, :] = (block * gain_ref[...]).astype(bf16)

        def columns(n, _):
            at = pl.multiple_of(n * TILE, TILE)
            for ref, base in ((gate_ref, 0), (up_ref, units)):
                value = dot(turned_ref[...], ref[:, pl.ds(at, TILE)]).astype(bf16)
                for d in range(size):
                    outs[d][:, pl.ds(pl.multiple_of(base + at, TILE), TILE)] = value[d * count : (d + 1) * count]
            return 0

        lax.fori_loop(0, units // TILE, columns, 0)

    return pl.pallas_call(
        body,
        out_shape=[jax.ShapeDtypeStruct((count, 2 * units + LANES), bf16)] * size,
        in_specs=[IN_SMEM] + [IN_VMEM] * 4,
        out_specs=[IN_VMEM] * size,
        scratch_shapes=[pltpu.VMEM((height, width), bf16)],
        compiler_params=pltpu.CompilerParams(vmem_limit_bytes=12 << 20),
        name="project",
    )(me, gain, rows, gate, up)


def lower_down(me, streams, matrix, shared, shared_matrix):
    size = len(streams[0][0])
    units = streams[0][0][0].shape[1]
    counts = [blocks[0].shape[0] for blocks, _ in streams]
    counts[-1] -= shared
    height = size * sum(counts)
    width = matrix.shape[1]

    def body(me_ref, *refs):
        matrix_ref, shared_ref, out_ref, shared_out_ref, rows_ref, shared_rows_ref = refs[size * len(counts) :]
        first = 0
        for i, count in enumerate(counts):
            flip = streams[i][1]
            for d in range(size):
                in_ref = refs[i * size + d]
                at = pl.multiple_of(first + block_row(me_ref[0], d, size, count, flip), 16)
                rows_ref[pl.ds(at, count), :] = in_ref[:count, :]
                if i == len(counts) - 1:
                    shared_rows_ref[pl.ds(block_row(me_ref[0], d, size, shared, flip), shared), :] = in_ref[count:, :]
            first += size * count

        def columns(n, _):
            at = pl.multiple_of(n * TILE, TILE)
            out_ref[:, pl.ds(at, TILE)] = dot(rows_ref[...], matrix_ref[:, pl.ds(at, TILE)]).astype(bf16)
            shared_out_ref[:, pl.ds(at, TILE)] = dot(shared_rows_ref[...], shared_ref[:, pl.ds(at, TILE)])
            return 0

        lax.fori_loop(0, width // TILE, columns, 0)

    return pl.pallas_call(
        body,
        out_shape=[jax.ShapeDtypeStruct((height, width), bf16), jax.ShapeDtypeStruct((size * shared, width), f32)],
        in_specs=[IN_SMEM] + [IN_VMEM] * (size * len(counts) + 2),
        out_specs=[IN_VMEM] * 2,
        scratch_shapes=[pltpu.VMEM((height, units), bf16), pltpu.VMEM((size * shared, units), bf16)],
        compiler_params=pltpu.CompilerParams(vmem_limit_bytes=14 << 20),
        name="lower_down",
    )(me, *[v for blocks, _ in streams for v in blocks], matrix, shared_matrix)


def layer(
    tokens,
    routes,
    route_weights,
    norm_gain,
    expert_gate,
    expert_up,
    expert_down,
    shared_gate,
    shared_up,
    shared_down,
    out_gain,
):
    tok_count, width = tokens.shape
    tp = lax.axis_size("tp")
    experts = lax.axis_size("ep")
    full_width = width * tp
    me_tp = lax.axis_index("tp")
    top_count = routes.shape[1]
    capacity = min(tok_count, 2 * tok_count * top_count // experts)
    gain = lax.dynamic_slice_in_dim(norm_gain, me_tp * width, width, 0)
    gate_matrix, up_matrix, down_matrix = expert_gate[0], expert_up[0], expert_down[0]
    hidden_units = gate_matrix.shape[1]

    expert_ids = lax.broadcasted_iota(jnp.int32, (1, 1, experts), 2)
    hit = routes[:, :, None] == expert_ids
    routed = jnp.any(hit, axis=1)
    weight = jnp.sum(jnp.where(hit, route_weights[:, :, None], 0.0), axis=1)
    lower = (
        lax.broadcasted_iota(jnp.int32, (tok_count, tok_count), 0)
        >= lax.broadcasted_iota(jnp.int32, (tok_count, tok_count), 1)
    ).astype(bf16)
    place = jnp.where(routed, dot(lower, routed.astype(bf16)) - 1.0, -1.0).astype(bf16)
    weight_high = weight.astype(bf16)
    weight_low = (weight - weight_high.astype(f32)).astype(bf16)

    columns = experts * capacity
    column = lax.broadcasted_iota(jnp.int32, (experts, columns), 1)
    expand = (column // capacity == lax.broadcasted_iota(jnp.int32, (experts, columns), 0)).astype(bf16)
    slot = (lax.broadcasted_iota(jnp.int32, (1, columns), 1) % capacity).astype(f32)
    pick = dot(place, expand) == slot
    high = jnp.where(pick, dot(weight_high, expand), 0.0).astype(bf16)
    low = jnp.where(pick, dot(weight_low, expand), 0.0).astype(bf16)

    def swapped(rows):
        return lax.all_to_all(rows.reshape(experts, capacity, width), "ep", 0, 0, tiled=True).reshape(columns, width)

    def hidden_of(total):
        scale = lax.rsqrt(total[:, 2 * hidden_units : 2 * hidden_units + 1] / full_width + epsilon)
        gate_value = total[:, :hidden_units] * scale
        up_value = total[:, hidden_units : 2 * hidden_units] * scale
        return (jax.nn.silu(gate_value) * up_value).astype(bf16)

    me = me_tp.reshape(1)
    gain = gain[None]
    leaving = lax.dot_general(pick.astype(bf16), tokens, (((0,), (0,)), ((), ())), preferred_element_type=f32)
    rows = swapped(leaving.astype(bf16))

    pieces_s = project(me, gain, tokens, 0, tok_count, shared_gate, shared_up, tp, False)
    hidden_s = hidden_of(reduce_scatter(pieces_s, tp, False, "tp"))
    rows, hidden_s = lax.optimization_barrier((rows, hidden_s))

    unit = 16 * tp
    units = columns // unit
    heights = [unit * (units * (i + 1) // STREAMS - units * i // STREAMS) for i in range(STREAMS)][::-1]
    totals = []
    for i, height in enumerate(heights):
        first, flip = sum(heights[:i]), i % 2 == 1
        pieces = project(me, gain, rows, first, height, gate_matrix, up_matrix, tp, flip)
        totals.append((reduce_scatter(pieces, tp, flip, "tp"), flip))
    streams = []
    for i, (total, flip) in enumerate(totals):
        hidden = hidden_of(total)
        if i == STREAMS - 1:
            hidden = jnp.concatenate([hidden, hidden_s], 0)
        streams.append((all_gather(hidden, tp, flip, "tp"), flip))
    down, shared_out = lower_down(me, streams, down_matrix, tok_count // tp, shared_down)
    came = swapped(down)
    mixture = shared_out + dot(high, came) + dot(low, came)

    square_sum = jnp.sum(mixture * mixture, axis=-1, keepdims=True)
    copies = jnp.broadcast_to(square_sum[None], (tp, *square_sum.shape))
    square_sum = lax.all_to_all(copies, "tp", 0, 0, tiled=True).sum(axis=0)
    scale = lax.rsqrt(square_sum / full_width + epsilon)
    return (mixture * scale * out_gain).astype(bf16)


def solution(mesh):
    return jax.shard_map(
        layer,
        mesh=mesh,
        in_specs=(
            P(("grp", "ep"), "tp"),
            P(("grp", "ep"), None),
            P(("grp", "ep"), None),
            P(),
            P("ep", "tp", None),
            P("ep", "tp", None),
            P("ep", None, "tp"),
            P("tp", None),
            P("tp", None),
            P(None, "tp"),
            P("tp"),
        ),
        out_specs=P(("grp", "ep"), "tp"),
        check_vma=False,
    )
```

```python
import jax
import jax.numpy as jnp
from jax import lax
from jax.experimental import pallas as pl
from jax.experimental.pallas import tpu as pltpu
from jax.sharding import PartitionSpec as P


epsilon = 1e-06
f32 = jnp.float32
bf16 = jnp.bfloat16


def dot(a, b):
    return jnp.dot(a, b, preferred_element_type=f32)


def exchanges(size, flip):
    pairs = [[(i, (i + (1 if i % 2 == way else -1)) % size) for i in range(size)] for way in (0, 1)]
    return pairs[::-1] if flip else pairs


def added(own, came):
    return (own.astype(f32) + came.astype(f32)).astype(bf16)


def reduce_scatter(piece, size, flip, axis):
    one, two = exchanges(size, flip)
    half = size // 2
    x = lax.ppermute(piece[half], axis, one)
    y = None
    for d in range(half - 1, 0, -1):
        x_next = added(piece[size - d] if (half - d) % 2 else piece[d], x)
        y_next = piece[d] if (half - d) % 2 else piece[size - d]
        y_next = y_next if y is None else added(y_next, y)
        x = lax.ppermute(x_next, axis, two if (half - d) % 2 else one)
        y = lax.ppermute(y_next, axis, one if (half - d) % 2 else two)
    return piece[0].astype(f32) + x.astype(f32) + y.astype(f32)


def all_gather(block, size, flip, axis):
    one, two = exchanges(size, flip)
    half = size // 2
    out = {0: block}
    x = y = block
    for d in range(1, half + 1):
        x = lax.ppermute(x, axis, two if d % 2 else one)
        out[size - d if d % 2 else d] = x
        if d < half:
            y = lax.ppermute(y, axis, one if d % 2 else two)
            out[d if d % 2 else size - d] = y
    return [out[d] for d in range(size)]


LANES = 128
TILE = 256
IN_VMEM = pl.BlockSpec()
IN_SMEM = pl.BlockSpec(memory_space=pltpu.SMEM)


def block_row(me, d, size, rows, flip):
    along = 1 - 2 * lax.rem(me, 2)
    return pl.multiple_of(lax.rem(me + size + (-d if flip else d) * along, size) * rows, 16)


def project(me, gain, rows, first, height, gate, up, size, flip):
    width = rows.shape[1]
    units = gate.shape[1]
    count = height // size

    def body(me_ref, gain_ref, rows_ref, gate_ref, up_ref, *refs):
        outs, turned_ref = refs[:-1], refs[-1]
        for d in range(size):
            at = pl.multiple_of(first + block_row(me_ref[0], d, size, count, flip), 16)
            block = rows_ref[pl.ds(at, count), :].astype(f32)
            squares = jnp.sum(block * block, axis=1, keepdims=True)
            outs[d][:, 2 * units :] = jnp.broadcast_to(squares, (count, LANES)).astype(bf16)
            turned_ref[d * count : (d + 1) * count, :] = (block * gain_ref[...]).astype(bf16)

        def columns(n, _):
            at = pl.multiple_of(n * TILE, TILE)
            for ref, base in ((gate_ref, 0), (up_ref, units)):
                value = dot(turned_ref[...], ref[:, pl.ds(at, TILE)]).astype(bf16)
                for d in range(size):
                    outs[d][:, pl.ds(pl.multiple_of(base + at, TILE), TILE)] = value[d * count : (d + 1) * count]
            return 0

        lax.fori_loop(0, units // TILE, columns, 0)

    return pl.pallas_call(
        body,
        out_shape=[jax.ShapeDtypeStruct((count, 2 * units + LANES), bf16)] * size,
        in_specs=[IN_SMEM] + [IN_VMEM] * 4,
        out_specs=[IN_VMEM] * size,
        scratch_shapes=[pltpu.VMEM((height, width), bf16)],
        compiler_params=pltpu.CompilerParams(vmem_limit_bytes=12 << 20),
        name="project",
    )(me, gain, rows, gate, up)


def lower_down(me, blocks_a, blocks_b, matrix, shared_matrix):
    size = len(blocks_a)
    count, units = blocks_a[0].shape
    shared = blocks_b[0].shape[0] - count
    width = matrix.shape[1]
    part = size * count

    def body(me_ref, *refs):
        ins_a, ins_b = refs[:size], refs[size : 2 * size]
        matrix_ref, shared_ref, out_ref, shared_out_ref, rows_ref, shared_rows_ref = refs[2 * size :]
        for d in range(size):
            at_a = block_row(me_ref[0], d, size, count, False)
            at_b = pl.multiple_of(part + block_row(me_ref[0], d, size, count, True), 16)
            at_s = block_row(me_ref[0], d, size, shared, True)
            rows_ref[pl.ds(at_a, count), :] = ins_a[d][...]
            rows_ref[pl.ds(at_b, count), :] = ins_b[d][:count, :]
            shared_rows_ref[pl.ds(at_s, shared), :] = ins_b[d][count:, :]

        def columns(n, _):
            at = pl.multiple_of(n * TILE, TILE)
            out_ref[:, pl.ds(at, TILE)] = dot(rows_ref[...], matrix_ref[:, pl.ds(at, TILE)]).astype(bf16)
            shared_out_ref[:, pl.ds(at, TILE)] = dot(shared_rows_ref[...], shared_ref[:, pl.ds(at, TILE)])
            return 0

        lax.fori_loop(0, width // TILE, columns, 0)

    return pl.pallas_call(
        body,
        out_shape=[jax.ShapeDtypeStruct((2 * part, width), bf16), jax.ShapeDtypeStruct((size * shared, width), f32)],
        in_specs=[IN_SMEM] + [IN_VMEM] * (2 * size + 2),
        out_specs=[IN_VMEM] * 2,
        scratch_shapes=[pltpu.VMEM((2 * part, units), bf16), pltpu.VMEM((size * shared, units), bf16)],
        compiler_params=pltpu.CompilerParams(vmem_limit_bytes=14 << 20),
        name="lower_down",
    )(me, *blocks_a, *blocks_b, matrix, shared_matrix)


def layer(
    tokens,
    routes,
    route_weights,
    norm_gain,
    expert_gate,
    expert_up,
    expert_down,
    shared_gate,
    shared_up,
    shared_down,
    out_gain,
):
    tok_count, width = tokens.shape
    tp = lax.axis_size("tp")
    experts = lax.axis_size("ep")
    full_width = width * tp
    me_tp = lax.axis_index("tp")
    top_count = routes.shape[1]
    capacity = min(tok_count, 2 * tok_count * top_count // experts)
    gain = lax.dynamic_slice_in_dim(norm_gain, me_tp * width, width, 0)
    gate_matrix, up_matrix, down_matrix = expert_gate[0], expert_up[0], expert_down[0]
    hidden_units = gate_matrix.shape[1]

    expert_ids = lax.broadcasted_iota(jnp.int32, (1, 1, experts), 2)
    hit = routes[:, :, None] == expert_ids
    routed = jnp.any(hit, axis=1)
    weight = jnp.sum(jnp.where(hit, route_weights[:, :, None], 0.0), axis=1)
    lower = (
        lax.broadcasted_iota(jnp.int32, (tok_count, tok_count), 0)
        >= lax.broadcasted_iota(jnp.int32, (tok_count, tok_count), 1)
    ).astype(bf16)
    place = jnp.where(routed, dot(lower, routed.astype(bf16)) - 1.0, -1.0).astype(bf16)
    weight_high = weight.astype(bf16)
    weight_low = (weight - weight_high.astype(f32)).astype(bf16)

    columns = experts * capacity
    column = lax.broadcasted_iota(jnp.int32, (experts, columns), 1)
    expand = (column // capacity == lax.broadcasted_iota(jnp.int32, (experts, columns), 0)).astype(bf16)
    slot = (lax.broadcasted_iota(jnp.int32, (1, columns), 1) % capacity).astype(f32)
    pick = dot(place, expand) == slot
    high = jnp.where(pick, dot(weight_high, expand), 0.0).astype(bf16)
    low = jnp.where(pick, dot(weight_low, expand), 0.0).astype(bf16)

    def swapped(rows):
        return lax.all_to_all(rows.reshape(experts, capacity, width), "ep", 0, 0, tiled=True).reshape(columns, width)

    def hidden_of(total):
        scale = lax.rsqrt(total[:, 2 * hidden_units : 2 * hidden_units + 1] / full_width + epsilon)
        gate_value = total[:, :hidden_units] * scale
        up_value = total[:, hidden_units : 2 * hidden_units] * scale
        return (jax.nn.silu(gate_value) * up_value).astype(bf16)

    me = me_tp.reshape(1)
    gain = gain[None]
    leaving = lax.dot_general(pick.astype(bf16), tokens, (((0,), (0,)), ((), ())), preferred_element_type=f32)
    rows = swapped(leaving.astype(bf16))

    pieces_s = project(me, gain, tokens, 0, tok_count, shared_gate, shared_up, tp, False)
    hidden_s = hidden_of(reduce_scatter(pieces_s, tp, False, "tp"))
    rows, hidden_s = lax.optimization_barrier((rows, hidden_s))

    part = columns // 2
    pieces_a = project(me, gain, rows, 0, part, gate_matrix, up_matrix, tp, False)
    pieces_b = project(me, gain, rows, part, part, gate_matrix, up_matrix, tp, True)
    total_a = reduce_scatter(pieces_a, tp, False, "tp")
    total_b = reduce_scatter(pieces_b, tp, True, "tp")
    blocks_a = all_gather(hidden_of(total_a), tp, False, "tp")
    blocks_b = all_gather(jnp.concatenate([hidden_of(total_b), hidden_s], 0), tp, True, "tp")
    down, shared_out = lower_down(me, blocks_a, blocks_b, down_matrix, shared_down)
    came = swapped(down)
    mixture = shared_out + dot(high, came) + dot(low, came)

    square_sum = jnp.sum(mixture * mixture, axis=-1, keepdims=True)
    copies = jnp.broadcast_to(square_sum[None], (tp, *square_sum.shape))
    square_sum = lax.all_to_all(copies, "tp", 0, 0, tiled=True).sum(axis=0)
    scale = lax.rsqrt(square_sum / full_width + epsilon)
    return (mixture * scale * out_gain).astype(bf16)


def solution(mesh):
    return jax.shard_map(
        layer,
        mesh=mesh,
        in_specs=(
            P(("grp", "ep"), "tp"),
            P(("grp", "ep"), None),
            P(("grp", "ep"), None),
            P(),
            P("ep", "tp", None),
            P("ep", "tp", None),
            P("ep", None, "tp"),
            P("tp", None),
            P("tp", None),
            P(None, "tp"),
            P("tp"),
        ),
        out_specs=P(("grp", "ep"), "tp"),
        check_vma=False,
    )
```

```python
import jax
import jax.numpy as jnp
from jax import lax
from jax.experimental import pallas as pl
from jax.experimental.pallas import tpu as pltpu
from jax.sharding import PartitionSpec as P


epsilon = 1e-06
f32 = jnp.float32
bf16 = jnp.bfloat16


def dot(a, b):
    return jnp.dot(a, b, preferred_element_type=f32)


def exchanges(size, flip):
    pairs = [[(i, (i + (1 if i % 2 == way else -1)) % size) for i in range(size)] for way in (0, 1)]
    return pairs[::-1] if flip else pairs


def added(own, came):
    return (own.astype(f32) + came.astype(f32)).astype(bf16)


def reduce_scatter(piece, size, flip, axis):
    one, two = exchanges(size, flip)
    half = size // 2
    x = lax.ppermute(piece[half], axis, one)
    y = None
    for d in range(half - 1, 0, -1):
        x_next = added(piece[size - d] if (half - d) % 2 else piece[d], x)
        y_next = piece[d] if (half - d) % 2 else piece[size - d]
        y_next = y_next if y is None else added(y_next, y)
        x = lax.ppermute(x_next, axis, two if (half - d) % 2 else one)
        y = lax.ppermute(y_next, axis, one if (half - d) % 2 else two)
    return piece[0].astype(f32) + x.astype(f32) + y.astype(f32)


def all_gather(block, size, flip, axis):
    one, two = exchanges(size, flip)
    half = size // 2
    out = {0: block}
    x = y = block
    for d in range(1, half + 1):
        x = lax.ppermute(x, axis, two if d % 2 else one)
        out[size - d if d % 2 else d] = x
        if d < half:
            y = lax.ppermute(y, axis, one if d % 2 else two)
            out[d if d % 2 else size - d] = y
    return [out[d] for d in range(size)]


LANES = 128
TILE = 256
IN_VMEM = pl.BlockSpec()
IN_SMEM = pl.BlockSpec(memory_space=pltpu.SMEM)


def block_row(me, d, size, rows, flip):
    along = 1 - 2 * lax.rem(me, 2)
    return pl.multiple_of(lax.rem(me + size + (-d if flip else d) * along, size) * rows, 16)


def project(me, gain, rows, first, height, gate, up, size, flip):
    width = rows.shape[1]
    units = gate.shape[1]
    count = height // size

    def body(me_ref, gain_ref, rows_ref, gate_ref, up_ref, *refs):
        outs, turned_ref = refs[:-1], refs[-1]
        for d in range(size):
            at = pl.multiple_of(first + block_row(me_ref[0], d, size, count, flip), 16)
            block = rows_ref[pl.ds(at, count), :].astype(f32)
            squares = jnp.sum(block * block, axis=1, keepdims=True)
            outs[d][:, 2 * units :] = jnp.broadcast_to(squares, (count, LANES)).astype(bf16)
            turned_ref[d * count : (d + 1) * count, :] = (block * gain_ref[...]).astype(bf16)

        def columns(n, _):
            at = pl.multiple_of(n * TILE, TILE)
            for ref, base in ((gate_ref, 0), (up_ref, units)):
                value = dot(turned_ref[...], ref[:, pl.ds(at, TILE)]).astype(bf16)
                for d in range(size):
                    outs[d][:, pl.ds(pl.multiple_of(base + at, TILE), TILE)] = value[d * count : (d + 1) * count]
            return 0

        lax.fori_loop(0, units // TILE, columns, 0)

    return pl.pallas_call(
        body,
        out_shape=[jax.ShapeDtypeStruct((count, 2 * units + LANES), bf16)] * size,
        in_specs=[IN_SMEM] + [IN_VMEM] * 4,
        out_specs=[IN_VMEM] * size,
        scratch_shapes=[pltpu.VMEM((height, width), bf16)],
        compiler_params=pltpu.CompilerParams(vmem_limit_bytes=12 << 20),
        name="project",
    )(me, gain, rows, gate, up)


def lower_down(me, streams, matrix, kind):
    size = len(streams[0][0])
    count, units = streams[0][0][0].shape
    part = size * count
    height = part * len(streams)
    width = matrix.shape[1]

    def body(me_ref, *refs):
        ins, (matrix_ref, out_ref, rows_ref) = refs[:-3], refs[-3:]
        for i, (_, flip) in enumerate(streams):
            for d in range(size):
                at = pl.multiple_of(i * part + block_row(me_ref[0], d, size, count, flip), 16)
                rows_ref[pl.ds(at, count), :] = ins[i * size + d][...]

        def columns(n, _):
            at = pl.multiple_of(n * TILE, TILE)
            out_ref[:, pl.ds(at, TILE)] = dot(rows_ref[...], matrix_ref[:, pl.ds(at, TILE)]).astype(kind)
            return 0

        lax.fori_loop(0, width // TILE, columns, 0)

    return pl.pallas_call(
        body,
        out_shape=jax.ShapeDtypeStruct((height, width), kind),
        in_specs=[IN_SMEM] + [IN_VMEM] * (size * len(streams) + 1),
        out_specs=IN_VMEM,
        scratch_shapes=[pltpu.VMEM((height, units), bf16)],
        compiler_params=pltpu.CompilerParams(vmem_limit_bytes=14 << 20),
        name="lower_down",
    )(me, *[v for blocks, _ in streams for v in blocks], matrix)


def layer(
    tokens,
    routes,
    route_weights,
    norm_gain,
    expert_gate,
    expert_up,
    expert_down,
    shared_gate,
    shared_up,
    shared_down,
    out_gain,
):
    tok_count, width = tokens.shape
    tp = lax.axis_size("tp")
    experts = lax.axis_size("ep")
    full_width = width * tp
    me_tp = lax.axis_index("tp")
    top_count = routes.shape[1]
    capacity = min(tok_count, 2 * tok_count * top_count // experts)
    gain = lax.dynamic_slice_in_dim(norm_gain, me_tp * width, width, 0)
    gate_matrix, up_matrix, down_matrix = expert_gate[0], expert_up[0], expert_down[0]
    hidden_units = gate_matrix.shape[1]

    expert_ids = lax.broadcasted_iota(jnp.int32, (1, 1, experts), 2)
    hit = routes[:, :, None] == expert_ids
    routed = jnp.any(hit, axis=1)
    weight = jnp.sum(jnp.where(hit, route_weights[:, :, None], 0.0), axis=1)
    lower = (
        lax.broadcasted_iota(jnp.int32, (tok_count, tok_count), 0)
        >= lax.broadcasted_iota(jnp.int32, (tok_count, tok_count), 1)
    ).astype(bf16)
    place = jnp.where(routed, dot(lower, routed.astype(bf16)) - 1.0, -1.0).astype(bf16)
    weight_high = weight.astype(bf16)
    weight_low = (weight - weight_high.astype(f32)).astype(bf16)

    columns = experts * capacity
    column = lax.broadcasted_iota(jnp.int32, (experts, columns), 1)
    expand = (column // capacity == lax.broadcasted_iota(jnp.int32, (experts, columns), 0)).astype(bf16)
    slot = (lax.broadcasted_iota(jnp.int32, (1, columns), 1) % capacity).astype(f32)
    pick = dot(place, expand) == slot
    high = jnp.where(pick, dot(weight_high, expand), 0.0).astype(bf16)
    low = jnp.where(pick, dot(weight_low, expand), 0.0).astype(bf16)

    def swapped(rows):
        return lax.all_to_all(rows.reshape(experts, capacity, width), "ep", 0, 0, tiled=True).reshape(columns, width)

    def hidden_of(total):
        scale = lax.rsqrt(total[:, 2 * hidden_units : 2 * hidden_units + 1] / full_width + epsilon)
        gate_value = total[:, :hidden_units] * scale
        up_value = total[:, hidden_units : 2 * hidden_units] * scale
        return (jax.nn.silu(gate_value) * up_value).astype(bf16)

    me = me_tp.reshape(1)
    gain = gain[None]
    leaving = lax.dot_general(pick.astype(bf16), tokens, (((0,), (0,)), ((), ())), preferred_element_type=f32)
    rows = swapped(leaving.astype(bf16))

    pieces_s = project(me, gain, tokens, 0, tok_count, shared_gate, shared_up, tp, False)
    hidden_s = hidden_of(reduce_scatter(pieces_s, tp, False, "tp"))
    rows, hidden_s = lax.optimization_barrier((rows, hidden_s))

    part = columns // 2
    pieces_a = project(me, gain, rows, 0, part, gate_matrix, up_matrix, tp, False)
    pieces_b = project(me, gain, rows, part, part, gate_matrix, up_matrix, tp, True)
    total_a = reduce_scatter(pieces_a, tp, False, "tp")
    total_b = reduce_scatter(pieces_b, tp, True, "tp")
    blocks_a = all_gather(hidden_of(total_a), tp, False, "tp")
    blocks_b = all_gather(hidden_of(total_b), tp, True, "tp")
    down = lower_down(me, [(blocks_a, False), (blocks_b, True)], down_matrix, bf16)
    came = swapped(down)
    blocks_s = all_gather(hidden_s, tp, False, "tp")
    shared_out = lower_down(me, [(blocks_s, False)], shared_down, f32)
    mixture = shared_out + dot(high, came) + dot(low, came)

    square_sum = jnp.sum(mixture * mixture, axis=-1, keepdims=True)
    copies = jnp.broadcast_to(square_sum[None], (tp, *square_sum.shape))
    square_sum = lax.all_to_all(copies, "tp", 0, 0, tiled=True).sum(axis=0)
    scale = lax.rsqrt(square_sum / full_width + epsilon)
    return (mixture * scale * out_gain).astype(bf16)


def solution(mesh):
    return jax.shard_map(
        layer,
        mesh=mesh,
        in_specs=(
            P(("grp", "ep"), "tp"),
            P(("grp", "ep"), None),
            P(("grp", "ep"), None),
            P(),
            P("ep", "tp", None),
            P("ep", "tp", None),
            P("ep", None, "tp"),
            P("tp", None),
            P("tp", None),
            P(None, "tp"),
            P("tp"),
        ),
        out_specs=P(("grp", "ep"), "tp"),
        check_vma=False,
    )
```

```python
import jax
import jax.numpy as jnp
from jax import lax
from jax.experimental import pallas as pl
from jax.experimental.pallas import tpu as pltpu
from jax.sharding import PartitionSpec as P


epsilon = 1e-06
f32 = jnp.float32
bf16 = jnp.bfloat16


def dot(a, b):
    return jnp.dot(a, b, preferred_element_type=f32)


def exchanges(size, flip):
    pairs = [[(i, (i + (1 if i % 2 == way else -1)) % size) for i in range(size)] for way in (0, 1)]
    return pairs[::-1] if flip else pairs


def added(own, came):
    return (own.astype(f32) + came.astype(f32)).astype(bf16)


def reduce_scatter(piece, size, flip, axis):
    one, two = exchanges(size, flip)
    half = size // 2
    x = lax.ppermute(piece[half], axis, one)
    y = None
    for d in range(half - 1, 0, -1):
        x_next = added(piece[size - d] if (half - d) % 2 else piece[d], x)
        y_next = piece[d] if (half - d) % 2 else piece[size - d]
        y_next = y_next if y is None else added(y_next, y)
        x = lax.ppermute(x_next, axis, two if (half - d) % 2 else one)
        y = lax.ppermute(y_next, axis, one if (half - d) % 2 else two)
    return piece[0].astype(f32) + x.astype(f32) + y.astype(f32)


def all_gather(block, size, flip, axis):
    one, two = exchanges(size, flip)
    half = size // 2
    out = {0: block}
    x = y = block
    for d in range(1, half + 1):
        x = lax.ppermute(x, axis, two if d % 2 else one)
        out[size - d if d % 2 else d] = x
        if d < half:
            y = lax.ppermute(y, axis, one if d % 2 else two)
            out[d if d % 2 else size - d] = y
    return [out[d] for d in range(size)]


LANES = 128
TILE = 256
IN_VMEM = pl.BlockSpec()
IN_SMEM = pl.BlockSpec(memory_space=pltpu.SMEM)


def block_row(me, d, size, rows, flip):
    along = 1 - 2 * lax.rem(me, 2)
    return pl.multiple_of(lax.rem(me + size + (-d if flip else d) * along, size) * rows, 16)


def project(me, gain, rows, first, height, gate, up, size, flip):
    width = rows.shape[1]
    units = gate.shape[1]
    count = height // size

    def body(me_ref, gain_ref, rows_ref, gate_ref, up_ref, *refs):
        outs, turned_ref = refs[:-1], refs[-1]
        for d in range(size):
            at = pl.multiple_of(first + block_row(me_ref[0], d, size, count, flip), 16)
            block = rows_ref[pl.ds(at, count), :].astype(f32)
            squares = jnp.sum(block * block, axis=1, keepdims=True)
            outs[d][:, 2 * units :] = jnp.broadcast_to(squares, (count, LANES)).astype(bf16)
            turned_ref[d * count : (d + 1) * count, :] = (block * gain_ref[...]).astype(bf16)

        def columns(n, _):
            at = pl.multiple_of(n * TILE, TILE)
            for ref, base in ((gate_ref, 0), (up_ref, units)):
                value = dot(turned_ref[...], ref[:, pl.ds(at, TILE)]).astype(bf16)
                for d in range(size):
                    outs[d][:, pl.ds(pl.multiple_of(base + at, TILE), TILE)] = value[d * count : (d + 1) * count]
            return 0

        lax.fori_loop(0, units // TILE, columns, 0)

    return pl.pallas_call(
        body,
        out_shape=[jax.ShapeDtypeStruct((count, 2 * units + LANES), bf16)] * size,
        in_specs=[IN_SMEM] + [IN_VMEM] * 4,
        out_specs=[IN_VMEM] * size,
        scratch_shapes=[pltpu.VMEM((height, width), bf16)],
        compiler_params=pltpu.CompilerParams(vmem_limit_bytes=12 << 20),
        name="project",
    )(me, gain, rows, gate, up)


def lower_down(me, blocks, flip, matrix, kind, above=()):
    size = len(blocks)
    count, units = blocks[0].shape
    height = size * count
    width = matrix.shape[1]
    first = sum(v.shape[0] for v in above)

    def body(me_ref, *refs):
        ins, matrix_ref, above_refs, (out_ref, rows_ref) = refs[:size], refs[size], refs[size + 1 : -2], refs[-2:]
        for d in range(size):
            rows_ref[pl.ds(block_row(me_ref[0], d, size, count, flip), count), :] = ins[d][...]
        for ref in above_refs:
            out_ref[:first, :] = ref[...]

        def columns(n, _):
            at = pl.multiple_of(n * TILE, TILE)
            out_ref[first:, pl.ds(at, TILE)] = dot(rows_ref[...], matrix_ref[:, pl.ds(at, TILE)]).astype(kind)
            return 0

        lax.fori_loop(0, width // TILE, columns, 0)

    return pl.pallas_call(
        body,
        out_shape=jax.ShapeDtypeStruct((first + height, width), kind),
        in_specs=[IN_SMEM] + [IN_VMEM] * (size + 1 + len(above)),
        out_specs=IN_VMEM,
        scratch_shapes=[pltpu.VMEM((height, units), bf16)],
        compiler_params=pltpu.CompilerParams(vmem_limit_bytes=12 << 20),
        name="lower_down",
    )(me, *blocks, matrix, *above)


def layer(
    tokens,
    routes,
    route_weights,
    norm_gain,
    expert_gate,
    expert_up,
    expert_down,
    shared_gate,
    shared_up,
    shared_down,
    out_gain,
):
    tok_count, width = tokens.shape
    tp = lax.axis_size("tp")
    experts = lax.axis_size("ep")
    full_width = width * tp
    me_tp = lax.axis_index("tp")
    top_count = routes.shape[1]
    capacity = min(tok_count, 2 * tok_count * top_count // experts)
    gain = lax.dynamic_slice_in_dim(norm_gain, me_tp * width, width, 0)
    gate_matrix, up_matrix, down_matrix = expert_gate[0], expert_up[0], expert_down[0]
    hidden_units = gate_matrix.shape[1]

    expert_ids = lax.broadcasted_iota(jnp.int32, (1, 1, experts), 2)
    hit = routes[:, :, None] == expert_ids
    routed = jnp.any(hit, axis=1)
    weight = jnp.sum(jnp.where(hit, route_weights[:, :, None], 0.0), axis=1)
    lower = (
        lax.broadcasted_iota(jnp.int32, (tok_count, tok_count), 0)
        >= lax.broadcasted_iota(jnp.int32, (tok_count, tok_count), 1)
    ).astype(bf16)
    place = jnp.where(routed, dot(lower, routed.astype(bf16)) - 1.0, -1.0).astype(bf16)
    weight_high = weight.astype(bf16)
    weight_low = (weight - weight_high.astype(f32)).astype(bf16)

    columns = experts * capacity
    column = lax.broadcasted_iota(jnp.int32, (experts, columns), 1)
    expand = (column // capacity == lax.broadcasted_iota(jnp.int32, (experts, columns), 0)).astype(bf16)
    slot = (lax.broadcasted_iota(jnp.int32, (1, columns), 1) % capacity).astype(f32)
    pick = dot(place, expand) == slot
    high = jnp.where(pick, dot(weight_high, expand), 0.0).astype(bf16)
    low = jnp.where(pick, dot(weight_low, expand), 0.0).astype(bf16)

    def swapped(rows):
        return lax.all_to_all(rows.reshape(experts, capacity, width), "ep", 0, 0, tiled=True).reshape(columns, width)

    def hidden_of(total):
        scale = lax.rsqrt(total[:, 2 * hidden_units : 2 * hidden_units + 1] / full_width + epsilon)
        gate_value = total[:, :hidden_units] * scale
        up_value = total[:, hidden_units : 2 * hidden_units] * scale
        return (jax.nn.silu(gate_value) * up_value).astype(bf16)

    me = me_tp.reshape(1)
    gain = gain[None]
    leaving = lax.dot_general(pick.astype(bf16), tokens, (((0,), (0,)), ((), ())), preferred_element_type=f32)
    rows = swapped(leaving.astype(bf16))

    pieces_s = project(me, gain, tokens, 0, tok_count, shared_gate, shared_up, tp, False)
    hidden_s = hidden_of(reduce_scatter(pieces_s, tp, False, "tp"))
    rows, hidden_s = lax.optimization_barrier((rows, hidden_s))

    part = columns // 2
    pieces_a = project(me, gain, rows, 0, part, gate_matrix, up_matrix, tp, False)
    pieces_b = project(me, gain, rows, part, part, gate_matrix, up_matrix, tp, True)
    total_a = reduce_scatter(pieces_a, tp, False, "tp")
    total_b = reduce_scatter(pieces_b, tp, True, "tp")
    blocks_a = all_gather(hidden_of(total_a), tp, False, "tp")
    blocks_b = all_gather(hidden_of(total_b), tp, False, "tp")
    down_a = lower_down(me, blocks_a, False, down_matrix, bf16)
    down = lower_down(me, blocks_b, False, down_matrix, bf16, above=(down_a,))
    came = swapped(down)
    blocks_s = all_gather(hidden_s, tp, False, "tp")
    shared_out = lower_down(me, blocks_s, False, shared_down, f32)
    mixture = shared_out + dot(high, came) + dot(low, came)

    square_sum = jnp.sum(mixture * mixture, axis=-1, keepdims=True)
    copies = jnp.broadcast_to(square_sum[None], (tp, *square_sum.shape))
    square_sum = lax.all_to_all(copies, "tp", 0, 0, tiled=True).sum(axis=0)
    scale = lax.rsqrt(square_sum / full_width + epsilon)
    return (mixture * scale * out_gain).astype(bf16)


def solution(mesh):
    return jax.shard_map(
        layer,
        mesh=mesh,
        in_specs=(
            P(("grp", "ep"), "tp"),
            P(("grp", "ep"), None),
            P(("grp", "ep"), None),
            P(),
            P("ep", "tp", None),
            P("ep", "tp", None),
            P("ep", None, "tp"),
            P("tp", None),
            P("tp", None),
            P(None, "tp"),
            P("tp"),
        ),
        out_specs=P(("grp", "ep"), "tp"),
        check_vma=False,
    )
```

```python
import jax
import jax.numpy as jnp
from jax import lax
from jax.experimental import pallas as pl
from jax.experimental.pallas import tpu as pltpu
from jax.sharding import PartitionSpec as P


epsilon = 1e-06
f32 = jnp.float32
bf16 = jnp.bfloat16


def dot(a, b):
    return jnp.dot(a, b, preferred_element_type=f32)


def exchanges(size, flip):
    pairs = [[(i, (i + (1 if i % 2 == way else -1)) % size) for i in range(size)] for way in (0, 1)]
    return pairs[::-1] if flip else pairs


def added(own, came):
    return (own.astype(f32) + came.astype(f32)).astype(bf16)


def reduce_scatter(piece, size, flip, axis):
    one, two = exchanges(size, flip)
    half = size // 2
    x = lax.ppermute(piece[half], axis, one)
    y = None
    for d in range(half - 1, 0, -1):
        x_next = added(piece[size - d] if (half - d) % 2 else piece[d], x)
        y_next = piece[d] if (half - d) % 2 else piece[size - d]
        y_next = y_next if y is None else added(y_next, y)
        x = lax.ppermute(x_next, axis, two if (half - d) % 2 else one)
        y = lax.ppermute(y_next, axis, one if (half - d) % 2 else two)
    return piece[0].astype(f32) + x.astype(f32) + y.astype(f32)


def all_gather(block, size, flip, axis):
    one, two = exchanges(size, flip)
    half = size // 2
    out = {0: block}
    x = y = block
    for d in range(1, half + 1):
        x = lax.ppermute(x, axis, two if d % 2 else one)
        out[size - d if d % 2 else d] = x
        if d < half:
            y = lax.ppermute(y, axis, one if d % 2 else two)
            out[d if d % 2 else size - d] = y
    return [out[d] for d in range(size)]


LANES = 128
TILE = 512
IN_VMEM = pl.BlockSpec()
IN_SMEM = pl.BlockSpec(memory_space=pltpu.SMEM)


def block_row(me, d, size, rows, flip):
    along = 1 - 2 * lax.rem(me, 2)
    return pl.multiple_of(lax.rem(me + size + (-d if flip else d) * along, size) * rows, 16)


def project(me, gain, rows, first, height, gate, up, size, flip):
    width = rows.shape[1]
    units = gate.shape[1]
    count = height // size

    def body(me_ref, gain_ref, rows_ref, gate_ref, up_ref, *refs):
        outs, turned_ref = refs[:-1], refs[-1]
        for d in range(size):
            at = pl.multiple_of(first + block_row(me_ref[0], d, size, count, flip), 16)
            block = rows_ref[pl.ds(at, count), :].astype(f32)
            squares = jnp.sum(block * block, axis=1, keepdims=True)
            outs[d][:, 2 * units :] = jnp.broadcast_to(squares, (count, LANES)).astype(bf16)
            turned_ref[d * count : (d + 1) * count, :] = (block * gain_ref[...]).astype(bf16)

        def columns(n, _):
            at = pl.multiple_of(n * TILE, TILE)
            for ref, base in ((gate_ref, 0), (up_ref, units)):
                value = dot(turned_ref[...], ref[:, pl.ds(at, TILE)]).astype(bf16)
                for d in range(size):
                    outs[d][:, pl.ds(pl.multiple_of(base + at, TILE), TILE)] = value[d * count : (d + 1) * count]
            return 0

        lax.fori_loop(0, units // TILE, columns, 0)

    return pl.pallas_call(
        body,
        out_shape=[jax.ShapeDtypeStruct((count, 2 * units + LANES), bf16)] * size,
        in_specs=[IN_SMEM] + [IN_VMEM] * 4,
        out_specs=[IN_VMEM] * size,
        scratch_shapes=[pltpu.VMEM((height, width), bf16)],
        compiler_params=pltpu.CompilerParams(vmem_limit_bytes=12 << 20),
        name="project",
    )(me, gain, rows, gate, up)


def lower_down(me, blocks, flip, matrix, kind, above=()):
    size = len(blocks)
    count, units = blocks[0].shape
    height = size * count
    width = matrix.shape[1]
    first = sum(v.shape[0] for v in above)

    def body(me_ref, *refs):
        ins, matrix_ref, above_refs, (out_ref, rows_ref) = refs[:size], refs[size], refs[size + 1 : -2], refs[-2:]
        for d in range(size):
            rows_ref[pl.ds(block_row(me_ref[0], d, size, count, flip), count), :] = ins[d][...]
        for ref in above_refs:
            out_ref[:first, :] = ref[...]

        def columns(n, _):
            at = pl.multiple_of(n * TILE, TILE)
            out_ref[first:, pl.ds(at, TILE)] = dot(rows_ref[...], matrix_ref[:, pl.ds(at, TILE)]).astype(kind)
            return 0

        lax.fori_loop(0, width // TILE, columns, 0)

    return pl.pallas_call(
        body,
        out_shape=jax.ShapeDtypeStruct((first + height, width), kind),
        in_specs=[IN_SMEM] + [IN_VMEM] * (size + 1 + len(above)),
        out_specs=IN_VMEM,
        scratch_shapes=[pltpu.VMEM((height, units), bf16)],
        compiler_params=pltpu.CompilerParams(vmem_limit_bytes=12 << 20),
        name="lower_down",
    )(me, *blocks, matrix, *above)


def layer(
    tokens,
    routes,
    route_weights,
    norm_gain,
    expert_gate,
    expert_up,
    expert_down,
    shared_gate,
    shared_up,
    shared_down,
    out_gain,
):
    tok_count, width = tokens.shape
    tp = lax.axis_size("tp")
    experts = lax.axis_size("ep")
    full_width = width * tp
    me_tp = lax.axis_index("tp")
    top_count = routes.shape[1]
    capacity = min(tok_count, 2 * tok_count * top_count // experts)
    gain = lax.dynamic_slice_in_dim(norm_gain, me_tp * width, width, 0)
    gate_matrix, up_matrix, down_matrix = expert_gate[0], expert_up[0], expert_down[0]
    hidden_units = gate_matrix.shape[1]

    expert_ids = lax.broadcasted_iota(jnp.int32, (1, 1, experts), 2)
    hit = routes[:, :, None] == expert_ids
    routed = jnp.any(hit, axis=1)
    weight = jnp.sum(jnp.where(hit, route_weights[:, :, None], 0.0), axis=1)
    lower = (
        lax.broadcasted_iota(jnp.int32, (tok_count, tok_count), 0)
        >= lax.broadcasted_iota(jnp.int32, (tok_count, tok_count), 1)
    ).astype(bf16)
    place = jnp.where(routed, dot(lower, routed.astype(bf16)) - 1.0, -1.0).astype(bf16)
    weight_high = weight.astype(bf16)
    weight_low = (weight - weight_high.astype(f32)).astype(bf16)

    columns = experts * capacity
    column = lax.broadcasted_iota(jnp.int32, (experts, columns), 1)
    expand = (column // capacity == lax.broadcasted_iota(jnp.int32, (experts, columns), 0)).astype(bf16)
    slot = (lax.broadcasted_iota(jnp.int32, (1, columns), 1) % capacity).astype(f32)
    pick = dot(place, expand) == slot
    high = jnp.where(pick, dot(weight_high, expand), 0.0).astype(bf16)
    low = jnp.where(pick, dot(weight_low, expand), 0.0).astype(bf16)

    def swapped(rows):
        return lax.all_to_all(rows.reshape(experts, capacity, width), "ep", 0, 0, tiled=True).reshape(columns, width)

    def hidden_of(total):
        scale = lax.rsqrt(total[:, 2 * hidden_units : 2 * hidden_units + 1] / full_width + epsilon)
        gate_value = total[:, :hidden_units] * scale
        up_value = total[:, hidden_units : 2 * hidden_units] * scale
        return (jax.nn.silu(gate_value) * up_value).astype(bf16)

    me = me_tp.reshape(1)
    gain = gain[None]
    spread = lax.dot_general(expand, place, (((0,), (1,)), ((), ())), preferred_element_type=f32)
    row_slot = (lax.broadcasted_iota(jnp.int32, (columns, 1), 0) % capacity).astype(f32)
    leaving = dot((spread == row_slot).astype(bf16), tokens)
    rows = swapped(leaving.astype(bf16))

    pieces_s = project(me, gain, tokens, 0, tok_count, shared_gate, shared_up, tp, False)
    hidden_s = hidden_of(reduce_scatter(pieces_s, tp, False, "tp"))
    rows, hidden_s = lax.optimization_barrier((rows, hidden_s))

    part = columns // 2
    pieces_a = project(me, gain, rows, 0, part, gate_matrix, up_matrix, tp, False)
    pieces_b = project(me, gain, rows, part, part, gate_matrix, up_matrix, tp, True)
    total_a = reduce_scatter(pieces_a, tp, False, "tp")
    total_b = reduce_scatter(pieces_b, tp, True, "tp")
    blocks_a = all_gather(hidden_of(total_a), tp, False, "tp")
    blocks_b = all_gather(hidden_of(total_b), tp, False, "tp")
    down_a = lower_down(me, blocks_a, False, down_matrix, bf16)
    down = lower_down(me, blocks_b, False, down_matrix, bf16, above=(down_a,))
    came = swapped(down)
    blocks_s = all_gather(hidden_s, tp, False, "tp")
    shared_out = lower_down(me, blocks_s, False, shared_down, f32)
    mixture = shared_out + dot(high, came) + dot(low, came)

    square_sum = jnp.sum(mixture * mixture, axis=-1, keepdims=True)
    copies = jnp.broadcast_to(square_sum[None], (tp, *square_sum.shape))
    square_sum = lax.all_to_all(copies, "tp", 0, 0, tiled=True).sum(axis=0)
    scale = lax.rsqrt(square_sum / full_width + epsilon)
    return (mixture * scale * out_gain).astype(bf16)


def solution(mesh):
    return jax.shard_map(
        layer,
        mesh=mesh,
        in_specs=(
            P(("grp", "ep"), "tp"),
            P(("grp", "ep"), None),
            P(("grp", "ep"), None),
            P(),
            P("ep", "tp", None),
            P("ep", "tp", None),
            P("ep", None, "tp"),
            P("tp", None),
            P("tp", None),
            P(None, "tp"),
            P("tp"),
        ),
        out_specs=P(("grp", "ep"), "tp"),
        check_vma=False,
    )
```

```python
import jax
import jax.numpy as jnp
from jax import lax
from jax.experimental import pallas as pl
from jax.experimental.pallas import tpu as pltpu
from jax.sharding import PartitionSpec as P


epsilon = 1e-06
f32 = jnp.float32
bf16 = jnp.bfloat16


def dot(a, b):
    return jnp.dot(a, b, preferred_element_type=f32)


def exchanges(size, flip):
    pairs = [[(i, (i + (1 if i % 2 == way else -1)) % size) for i in range(size)] for way in (0, 1)]
    return pairs[::-1] if flip else pairs


def added(own, came):
    return (own.astype(f32) + came.astype(f32)).astype(bf16)


def reduce_scatter(piece, size, flip, axis):
    one, two = exchanges(size, flip)
    half = size // 2
    x = lax.ppermute(piece[half], axis, one)
    y = None
    for d in range(half - 1, 0, -1):
        x_next = added(piece[size - d] if (half - d) % 2 else piece[d], x)
        y_next = piece[d] if (half - d) % 2 else piece[size - d]
        y_next = y_next if y is None else added(y_next, y)
        x = lax.ppermute(x_next, axis, two if (half - d) % 2 else one)
        y = lax.ppermute(y_next, axis, one if (half - d) % 2 else two)
    return piece[0].astype(f32) + x.astype(f32) + y.astype(f32)


def all_gather(block, size, flip, axis):
    one, two = exchanges(size, flip)
    half = size // 2
    out = {0: block}
    x = y = block
    for d in range(1, half + 1):
        x = lax.ppermute(x, axis, two if d % 2 else one)
        out[size - d if d % 2 else d] = x
        if d < half:
            y = lax.ppermute(y, axis, one if d % 2 else two)
            out[d if d % 2 else size - d] = y
    return [out[d] for d in range(size)]


LANES = 128
TILE = 512
IN_VMEM = pl.BlockSpec()
IN_SMEM = pl.BlockSpec(memory_space=pltpu.SMEM)


def block_row(me, d, size, rows, flip):
    along = 1 - 2 * lax.rem(me, 2)
    return pl.multiple_of(lax.rem(me + size + (-d if flip else d) * along, size) * rows, 16)


def project(me, gain, rows, first, height, gate, up, size, flip):
    width = rows.shape[1]
    units = gate.shape[1]
    count = height // size

    def body(me_ref, gain_ref, rows_ref, gate_ref, up_ref, *refs):
        outs, turned_ref = refs[:-1], refs[-1]
        for d in range(size):
            at = pl.multiple_of(first + block_row(me_ref[0], d, size, count, flip), 16)
            block = rows_ref[pl.ds(at, count), :].astype(f32)
            squares = jnp.sum(block * block, axis=1, keepdims=True)
            outs[d][:, 2 * units :] = jnp.broadcast_to(squares, (count, LANES)).astype(bf16)
            turned_ref[d * count : (d + 1) * count, :] = (block * gain_ref[...]).astype(bf16)

        def columns(n, _):
            at = pl.multiple_of(n * TILE, TILE)
            for ref, base in ((gate_ref, 0), (up_ref, units)):
                value = dot(turned_ref[...], ref[:, pl.ds(at, TILE)]).astype(bf16)
                for d in range(size):
                    outs[d][:, pl.ds(pl.multiple_of(base + at, TILE), TILE)] = value[d * count : (d + 1) * count]
            return 0

        lax.fori_loop(0, units // TILE, columns, 0)

    return pl.pallas_call(
        body,
        out_shape=[jax.ShapeDtypeStruct((count, 2 * units + LANES), bf16)] * size,
        in_specs=[IN_SMEM] + [IN_VMEM] * 4,
        out_specs=[IN_VMEM] * size,
        scratch_shapes=[pltpu.VMEM((height, width), bf16)],
        compiler_params=pltpu.CompilerParams(vmem_limit_bytes=12 << 20),
        name="project",
    )(me, gain, rows, gate, up)


def lower_down(me, blocks, flip, matrix, kind, below=()):
    size = len(blocks)
    count, units = blocks[0].shape
    height = size * count
    width = matrix.shape[1]
    rest = sum(v.shape[0] for v in below)

    def body(me_ref, *refs):
        ins, matrix_ref, below_refs, (out_ref, rows_ref) = refs[:size], refs[size], refs[size + 1 : -2], refs[-2:]
        for d in range(size):
            rows_ref[pl.ds(block_row(me_ref[0], d, size, count, flip), count), :] = ins[d][...]
        for ref in below_refs:
            out_ref[height:, :] = ref[...]

        def columns(n, _):
            at = pl.multiple_of(n * TILE, TILE)
            out_ref[:height, pl.ds(at, TILE)] = dot(rows_ref[...], matrix_ref[:, pl.ds(at, TILE)]).astype(kind)
            return 0

        lax.fori_loop(0, width // TILE, columns, 0)

    return pl.pallas_call(
        body,
        out_shape=jax.ShapeDtypeStruct((height + rest, width), kind),
        in_specs=[IN_SMEM] + [IN_VMEM] * (size + 1 + len(below)),
        out_specs=IN_VMEM,
        scratch_shapes=[pltpu.VMEM((height, units), bf16)],
        compiler_params=pltpu.CompilerParams(vmem_limit_bytes=12 << 20),
        name="lower_down",
    )(me, *blocks, matrix, *below)


def layer(
    tokens,
    routes,
    route_weights,
    norm_gain,
    expert_gate,
    expert_up,
    expert_down,
    shared_gate,
    shared_up,
    shared_down,
    out_gain,
):
    tok_count, width = tokens.shape
    tp = lax.axis_size("tp")
    experts = lax.axis_size("ep")
    full_width = width * tp
    me_tp = lax.axis_index("tp")
    top_count = routes.shape[1]
    capacity = min(tok_count, 2 * tok_count * top_count // experts)
    gain = lax.dynamic_slice_in_dim(norm_gain, me_tp * width, width, 0)
    gate_matrix, up_matrix, down_matrix = expert_gate[0], expert_up[0], expert_down[0]
    hidden_units = gate_matrix.shape[1]

    expert_ids = lax.broadcasted_iota(jnp.int32, (1, 1, experts), 2)
    hit = routes[:, :, None] == expert_ids
    routed = jnp.any(hit, axis=1)
    weight = jnp.sum(jnp.where(hit, route_weights[:, :, None], 0.0), axis=1)
    lower = (
        lax.broadcasted_iota(jnp.int32, (tok_count, tok_count), 0)
        >= lax.broadcasted_iota(jnp.int32, (tok_count, tok_count), 1)
    ).astype(bf16)
    place = jnp.where(routed, dot(lower, routed.astype(bf16)) - 1.0, -1.0).astype(bf16)
    weight_high = weight.astype(bf16)
    weight_low = (weight - weight_high.astype(f32)).astype(bf16)

    columns = experts * capacity
    column = lax.broadcasted_iota(jnp.int32, (experts, columns), 1)
    expand = (column // capacity == lax.broadcasted_iota(jnp.int32, (experts, columns), 0)).astype(bf16)
    slot = (lax.broadcasted_iota(jnp.int32, (1, columns), 1) % capacity).astype(f32)
    pick = dot(place, expand) == slot
    high = jnp.where(pick, dot(weight_high, expand), 0.0).astype(bf16)
    low = jnp.where(pick, dot(weight_low, expand), 0.0).astype(bf16)

    def swapped(rows):
        return lax.all_to_all(rows.reshape(experts, capacity, width), "ep", 0, 0, tiled=True).reshape(columns, width)

    def hidden_of(total):
        scale = lax.rsqrt(total[:, 2 * hidden_units : 2 * hidden_units + 1] / full_width + epsilon)
        gate_value = total[:, :hidden_units] * scale
        up_value = total[:, hidden_units : 2 * hidden_units] * scale
        return (jax.nn.silu(gate_value) * up_value).astype(bf16)

    me = me_tp.reshape(1)
    gain = gain[None]
    leaving = lax.dot_general(pick.astype(bf16), tokens, (((0,), (0,)), ((), ())), preferred_element_type=f32)
    rows = swapped(leaving.astype(bf16))

    pieces_s = project(me, gain, tokens, 0, tok_count, shared_gate, shared_up, tp, False)
    hidden_s = hidden_of(reduce_scatter(pieces_s, tp, False, "tp"))
    rows, hidden_s = lax.optimization_barrier((rows, hidden_s))

    part = columns // 2
    pieces_a = project(me, gain, rows, 0, part, gate_matrix, up_matrix, tp, False)
    pieces_b = project(me, gain, rows, part, part, gate_matrix, up_matrix, tp, True)
    total_a = reduce_scatter(pieces_a, tp, False, "tp")
    total_b = reduce_scatter(pieces_b, tp, True, "tp")
    blocks_a = all_gather(hidden_of(total_a), tp, False, "tp")
    blocks_b = all_gather(hidden_of(total_b), tp, False, "tp")
    down_b = lower_down(me, blocks_b, False, down_matrix, bf16)
    down = lower_down(me, blocks_a, False, down_matrix, bf16, below=(down_b,))
    came = swapped(down)
    blocks_s = all_gather(hidden_s, tp, False, "tp")
    shared_out = lower_down(me, blocks_s, False, shared_down, f32)
    mixture = shared_out + dot(high, came) + dot(low, came)

    square_sum = jnp.sum(mixture * mixture, axis=-1, keepdims=True)
    copies = jnp.broadcast_to(square_sum[None], (tp, *square_sum.shape))
    square_sum = lax.all_to_all(copies, "tp", 0, 0, tiled=True).sum(axis=0)
    scale = lax.rsqrt(square_sum / full_width + epsilon)
    return (mixture * scale * out_gain).astype(bf16)


def solution(mesh):
    return jax.shard_map(
        layer,
        mesh=mesh,
        in_specs=(
            P(("grp", "ep"), "tp"),
            P(("grp", "ep"), None),
            P(("grp", "ep"), None),
            P(),
            P("ep", "tp", None),
            P("ep", "tp", None),
            P("ep", None, "tp"),
            P("tp", None),
            P("tp", None),
            P(None, "tp"),
            P("tp"),
        ),
        out_specs=P(("grp", "ep"), "tp"),
        check_vma=False,
    )
```
